512 devices in a mesh: fs: 64 (over z, y), tp: 8 (over x, core).
Axes of the slice: x: 4, y: 8, z: 8, core: 2. Of those that a mesh axis runs over, the one named last changes fastest.
Arguments:
- tokens: bfloat16 [16384, 2048], P('fs', 'tp'), may hold values from -6 to 6
- mixer_norm_gain: bfloat16 [2048], replicated, may hold values from 0.099609375 to 1.8984375
- recurrence_branch_weight: bfloat16 [2048, 1024], P('fs', 'tp'), may hold values from -0.125 to 0.125
- output_gate_projection: bfloat16 [2048, 1024], P('fs', 'tp'), may hold values from -0.125 to 0.125
- recurrence_conv_taps: bfloat16 [4, 1024], P(None, 'tp'), may hold values from -3 to 3
- recurrence_gate_map: bfloat16 [16, 64, 64], P('tp'), may hold values from -0.75 to 0.75
- input_gate_map: bfloat16 [16, 64, 64], P('tp'), may hold values from -0.75 to 0.75
- channel_decay_rate: float32 [1024], P('tp'), may hold values from 0.001 to 0.03
- position_log_decay: float32 [16384, 1024], P('fs', 'tp'), may hold values from -0.69 to 0
- mixer_output_weight: bfloat16 [1024, 2048], P('tp', 'fs'), may hold values from -0.75 to 0.75
- feedforward_norm_gain: bfloat16 [2048], replicated, may hold values from 0.099609375 to 1.8984375
- gate_up_weight: bfloat16 [2048, 5632], P('fs', 'tp'), may hold values from -0.125 to 0.125
- value_up_weight: bfloat16 [2048, 5632], P('fs', 'tp'), may hold values from -0.125 to 0.125
- gate_conv_taps: bfloat16 [3, 5632], P(None, 'tp'), may hold values from -3 to 3
- value_conv_taps: bfloat16 [3, 5632], P(None, 'tp'), may hold values from -3 to 3
- down_projection_weight: bfloat16 [5632, 2048], P('tp', 'fs'), may hold values from -0.15625 to 0.15625
Outputs:
- result: bfloat16 [16384, 2048], P('fs', 'tp')
The draws below stay inside these ranges and needn't reach their ends.
All inputs are finite; a program needn't handle non-finite values.
Results may differ from the reference program's by a relative error of at most 0.024.
Values may be sent and summed in bfloat16 or wider, within the bound.
A program may use at most 64 MiB of HBM per device.

```python
import math
import jax
import jax.numpy as jnp
from jax import lax

D = 2048
HEADS = 16
HEAD_DIM = 64
W = 1024
FF = 5632
SEQ_LEN = 64
TOKENS = 16384
N_TP = 8


def draw_channel_decay_rate(key, part):
    base = jax.random.fold_in(key, 17)
    key_pick, key_slow, key_fast = jax.random.split(base, 3)
    limit = 5
    picked = jax.random.randint(key_pick, (W,), 0, 10) < limit
    slow_rate = jnp.exp(jax.random.uniform(key_slow, (W,), jnp.float32, math.log(0.001), math.log(0.004)))
    fast_rate = jnp.exp(jax.random.uniform(key_fast, (W,), jnp.float32, math.log(0.012), math.log(0.03)))
    return jnp.where(picked, slow_rate, fast_rate).astype(jnp.float32)


def draw_position_log_decay(key, part):
    base = jax.random.fold_in(key, 29)
    key_marks, key_depth = jax.random.split(base, 2)
    marks = (jax.random.randint(key_marks, (TOKENS, 1), 0, 32) == 0).astype(jnp.float32)
    depth = jax.random.uniform(key_depth, (TOKENS, W), jnp.float32, 0.22, 0.69)
    return (-marks * depth).astype(jnp.float32)


def steps_of(rng, extent, pieces, low, top_value):
    level, own = 1.0, jax.random.fold_in(rng, 6)
    for position, parts in pieces:
        steps = jnp.exp(jax.random.uniform(jax.random.fold_in(own, position), (parts,), jnp.float32, low / len(pieces), top_value / len(pieces)))
        level = level * jnp.repeat(steps, extent[position] // parts).reshape([-1 if axis == position else 1 for axis in range(len(extent))])
    return level


def normal_values(stream_key, extent, scale, most, shards=(), dtype=jnp.bfloat16):
    drawn = jax.random.normal(stream_key, extent, jnp.float32) * scale
    if len(shards) > 0:
        drawn = steps_of(stream_key, extent, shards, -0.22, 0.18) * drawn
    return jnp.clip(drawn, min=-most, max=most).astype(dtype)


def setup_inputs(seed: int = 0) -> dict:
    key_list = jax.random.split(jax.random.key(seed), 17)
    tokens = normal_values(key_list[0], (TOKENS, D), 1.0, 6.0, ((0, 64), (1, 8)))
    mixer_norm_gain = jnp.clip(1.0 + 0.18 * jax.random.normal(key_list[1], (D,), jnp.float32), 0.099609375, 1.8984375).astype(jnp.bfloat16)
    recurrence_branch_weight = normal_values(key_list[2], (D, W), D ** -0.5, 0.125, ((0, 64), (1, 8)))
    output_gate_projection = normal_values(key_list[3], (D, W), D ** -0.5, 0.125, ((0, 64), (1, 8)))
    recurrence_conv_taps = normal_values(key_list[4], (4, W), 0.5, 3.0, ((1, 8),))
    recurrence_gate_map = normal_values(key_list[5], (HEADS, HEAD_DIM, HEAD_DIM), HEAD_DIM ** -0.5, 0.75, ((0, 8),))
    input_gate_map = normal_values(key_list[6], (HEADS, HEAD_DIM, HEAD_DIM), HEAD_DIM ** -0.5, 0.75, ((0, 8),))
    channel_decay_rate = draw_channel_decay_rate(jax.random.fold_in(key_list[16], 71), 0)
    position_log_decay = draw_position_log_decay(jax.random.fold_in(key_list[16], 71), 0)
    mixer_output_weight = normal_values(key_list[9], (W, D), (W // 16) ** -0.5, 0.75, ((0, 8), (1, 64)))
    feedforward_norm_gain = jnp.clip(1.0 + 0.18 * jax.random.normal(key_list[10], (D,), jnp.float32), 0.099609375, 1.8984375).astype(jnp.bfloat16)
    gate_up_weight = normal_values(key_list[11], (D, FF), D ** -0.5, 0.125, ((0, 64), (1, 8)))
    value_up_weight = normal_values(key_list[12], (D, FF), D ** -0.5, 0.125, ((0, 64), (1, 8)))
    gate_conv_taps = normal_values(key_list[13], (3, FF), 0.6, 3.0, ((1, 8),))
    value_conv_taps = normal_values(key_list[14], (3, FF), 0.6, 3.0, ((1, 8),))
    down_projection_weight = normal_values(key_list[15], (FF, D), (FF // 4) ** -0.5, 0.15625, ((0, 8), (1, 64)))
    return {"tokens": tokens, "mixer_norm_gain": mixer_norm_gain, "recurrence_branch_weight": recurrence_branch_weight, "output_gate_projection": output_gate_projection, "recurrence_conv_taps": recurrence_conv_taps, "recurrence_gate_map": recurrence_gate_map, "input_gate_map": input_gate_map, "channel_decay_rate": channel_decay_rate, "position_log_decay": position_log_decay, "mixer_output_weight": mixer_output_weight, "feedforward_norm_gain": feedforward_norm_gain, "gate_up_weight": gate_up_weight, "value_up_weight": value_up_weight, "gate_conv_taps": gate_conv_taps, "value_conv_taps": value_conv_taps, "down_projection_weight": down_projection_weight}


EPS = 1e-06
DECAY_RATE_GAIN = 8.0

def rms_normed(values, gain):
    wide = values.astype(jnp.float32)
    factor = lax.rsqrt(lax.optimization_barrier(jnp.mean(wide * wide, axis=-1, keepdims=True)) + EPS)
    return (wide * factor * gain.astype(jnp.float32)).astype(jnp.bfloat16)

def causal_conv(values, kernel):
    width = kernel.shape[0]
    row_count, channels = values.shape
    grouped = values.astype(jnp.float32).reshape(row_count // SEQ_LEN, SEQ_LEN, channels)
    padded = jnp.pad(grouped, ((0, 0), (width - 1, 0), (0, 0)))
    summed = padded[:, 0:SEQ_LEN] * kernel[0].astype(jnp.float32)
    for offset in range(1, width):
        summed = summed + padded[:, offset:offset + SEQ_LEN] * kernel[offset].astype(jnp.float32)
    return summed.reshape(row_count, channels)

def combine(left, right):
    first_a, first_b = left
    second_a, second_b = right
    return (first_a * second_a, second_a * first_b + second_b)

def block_sums(left, weight, blocks):
    width = left.shape[1] // blocks
    summed = jnp.zeros((left.shape[0], weight.shape[1]), jnp.float32)
    for index in range(blocks):
        partial_sum = jnp.dot(left[:, index * width:(index + 1) * width], weight[index * width:(index + 1) * width], preferred_element_type=jnp.float32)
        summed = summed + partial_sum.astype(jnp.bfloat16).astype(jnp.float32)
    return summed

def reference(tokens, mixer_norm_gain, recurrence_branch_weight, output_gate_projection, recurrence_conv_taps, recurrence_gate_map, input_gate_map, channel_decay_rate, position_log_decay, mixer_output_weight, feedforward_norm_gain, gate_up_weight, value_up_weight, gate_conv_taps, value_conv_taps, down_projection_weight):
    row_count = tokens.shape[0]
    normed = rms_normed(tokens, mixer_norm_gain)
    branch = jnp.dot(normed, recurrence_branch_weight, preferred_element_type=jnp.float32).astype(jnp.bfloat16)
    outgate = jnp.dot(normed, output_gate_projection, preferred_element_type=jnp.float32).astype(jnp.bfloat16)
    conv = causal_conv(branch, recurrence_conv_taps).astype(jnp.bfloat16)
    grouped = conv.astype(jnp.float32).reshape(row_count, HEADS, HEAD_DIM)
    recurrence_scan = jax.nn.sigmoid(jnp.einsum('rhi,hij->rhj', grouped, recurrence_gate_map.astype(jnp.float32)).reshape(row_count, W))
    inner = jax.nn.sigmoid(jnp.einsum('rhi,hij->rhj', grouped, input_gate_map.astype(jnp.float32)).reshape(row_count, W))
    log_alpha = -DECAY_RATE_GAIN * recurrence_scan * channel_decay_rate[None, :] + position_log_decay
    drive = jnp.sqrt(-jnp.expm1(2.0 * log_alpha)) * inner * conv.astype(jnp.float32)
    shape3 = (row_count // SEQ_LEN, SEQ_LEN, W)
    unused, state = lax.associative_scan(combine, (jnp.exp(log_alpha).reshape(shape3), drive.reshape(shape3)), axis=1)
    state = state.reshape(row_count, W)
    mixed = (state * jax.nn.gelu(outgate.astype(jnp.float32))).astype(jnp.bfloat16)
    after = (tokens.astype(jnp.float32) + block_sums(mixed, mixer_output_weight, N_TP)).astype(jnp.bfloat16)
    normed2 = rms_normed(after, feedforward_norm_gain)
    gate_half = jnp.dot(normed2, gate_up_weight, preferred_element_type=jnp.float32).astype(jnp.bfloat16)
    value_half = jnp.dot(normed2, value_up_weight, preferred_element_type=jnp.float32).astype(jnp.bfloat16)
    hidden = (jax.nn.silu(causal_conv(gate_half, gate_conv_taps)) * causal_conv(value_half, value_conv_taps)).astype(jnp.bfloat16)
    return (after.astype(jnp.float32) + block_sums(hidden, down_projection_weight, N_TP)).astype(jnp.bfloat16)
```

```python
import functools

import jax
import jax.numpy as jnp
from jax import lax
from jax.experimental import pallas as pl
from jax.experimental.pallas import tpu as pltpu
from jax.sharding import Mesh
from jax.sharding import PartitionSpec as P

SEQ = 64
FS = ("fs_0", "fs_1")
EPS = 1e-06
DECAY_RATE_GAIN = 8.0
BF = jnp.bfloat16
F32 = jnp.float32
MESH = pl.DeviceIdType.MESH
N = 8
X = 4
MESSAGES = 240


def f32(v):
    return v.astype(F32)


def dot(a, b):
    return jnp.dot(a, b, preferred_element_type=F32)


def dot_t(a, b):
    return lax.dot_general(a, b, (((1,), (1,)), ((), ())), preferred_element_type=F32)


def place(offset):
    r = lax.broadcasted_iota(jnp.int32, (64, 128), 0)
    c = lax.broadcasted_iota(jnp.int32, (64, 128), 1)
    return jnp.where(c == r + offset, 1.0, 0.0).astype(BF)


def shifted(v, k, row, fill=0.0):
    return jnp.where(row >= k, pltpu.roll(v, k, 0), fill)


def conv(v, taps, row):
    width = taps.shape[0]
    total = v * taps[width - 1 : width]
    for k in range(1, width):
        total = total + shifted(v, k, row) * taps[width - 1 - k : width - k]
    return total


class Wire:
    def __init__(self, send, recv):
        self.send_sem, self.recv_sem, self.copies = send, recv, {}

    def go(self, key, src, dst, dev):
        k = len(self.copies)
        copy = pltpu.make_async_remote_copy(
            src_ref=src,
            dst_ref=dst,
            send_sem=self.send_sem.at[k],
            recv_sem=self.recv_sem.at[k],
            device_id=dev,
            device_id_type=MESH,
        )
        copy.start()
        self.copies[key] = copy

    def got(self, key):
        self.copies[key].wait_recv()

    def finish(self):
        for copy in self.copies.values():
            copy.wait_send()


class Spread:
    def __init__(self, wire, name, index, buf, chunks, here):
        self.wire, self.name, self.index, self.buf, self.chunks = wire, name, index, buf, chunks
        self.z, self.y, self.t = here

    def neighbour(self, axis, way):
        if axis == 0:
            return (lax.rem(self.z + N + way, N), self.y, self.t)
        return (self.z, lax.rem(self.y + N + way, N), self.t)

    def first(self, half, way, step):
        axis = 1 - half
        pos = lax.rem((self.y if axis else self.z) + N - way * (step - 1), N)
        return self.buf.at[self.z, pos, 0] if half == 0 else self.buf.at[pos, self.y, 1]

    def steps1(self, half, way):
        far = 1 if (self.index + half) % 2 == 0 else -1
        return N // 2 if way == far else N // 2 - 1

    def send1(self, step):
        for half in (0, 1):
            for way in (1, -1):
                if step <= self.steps1(half, way):
                    ref = self.first(half, way, step)
                    self.wire.go((self.name, 1, half, way, step), ref, ref, self.neighbour(1 - half, way))

    def forward1(self, step):
        for half in (0, 1):
            for way in (1, -1):
                if step <= self.steps1(half, way):
                    self.wire.got((self.name, 1, half, way, step))
                if step + 1 <= self.steps1(half, way):
                    ref = self.first(half, way, step + 1)
                    self.wire.go(
                        (self.name, 1, half, way, step + 1), ref, ref, self.neighbour(1 - half, way)
                    )

    def second(self, half, way, step, q):
        size = N // self.chunks
        pos = lax.rem((self.y if half else self.z) + N - way * (step - 1), N)
        part = pl.ds(q * size, size)
        return self.buf.at[pos, part, 0] if half == 0 else self.buf.at[part, pos, 1]

    def steps2(self, way, q):
        far = 1 if q < self.chunks // 2 else -1
        return N // 2 if way == far else N // 2 - 1

    def send2(self, q):
        for half in (0, 1):
            for way in (1, -1):
                ref = self.second(half, way, 1, q)
                self.wire.go((self.name, 2, half, way, 1, q), ref, ref, self.neighbour(half, way))

    def forward2(self, q, step):
        for half in (0, 1):
            for way in (1, -1):
                if step <= self.steps2(way, q):
                    self.wire.got((self.name, 2, half, way, step, q))
                if step + 1 <= self.steps2(way, q):
                    ref = self.second(half, way, step + 1, q)
                    self.wire.go(
                        (self.name, 2, half, way, step + 1, q), ref, ref, self.neighbour(half, way)
                    )


class Row:
    def __init__(self, z, y, t):
        self.z, self.y, self.t = z, y, t
        self.x, self.c = t // 2, lax.rem(t, 2)
        self.right = lax.rem(self.x + 1, X)
        self.left = lax.rem(self.x + X - 1, X)
        self.across = lax.rem(self.x + 2, X)

    def dev(self, x):
        return (self.z, self.y, 2 * x + self.c)

    def same(self, x):
        return 2 * x + self.c

    @property
    def partner(self):
        return (self.z, self.y, 2 * self.x + 1 - self.c)


class Gather:
    def __init__(self, wire, name, buf, row):
        self.wire, self.name, self.buf, self.row = wire, name, buf, row

    def key(self, *k):
        return (self.name, *k)

    def start(self):
        r, b = self.row, self.buf
        for k in (0, 1):
            for way, x in ((1, r.right), (-1, r.left)):
                half = k if way == 1 else 1 - k
                ref = b.at[r.t, half]
                self.wire.go(self.key("near", way, half), ref, ref, r.dev(x))
        self.wire.go(self.key("own"), b.at[r.t], b.at[r.t], r.partner)

    def relay(self):
        r, b = self.row, self.buf
        self.wire.got(self.key("near", 1, 0))
        ref = b.at[r.same(r.left), 0]
        self.wire.go(self.key("far", 1), ref, ref, r.dev(r.right))
        self.wire.got(self.key("near", -1, 1))
        ref = b.at[r.same(r.right), 1]
        self.wire.go(self.key("far", -1), ref, ref, r.dev(r.left))

    def share(self):
        r, b = self.row, self.buf
        self.wire.got(self.key("near", 1, 1))
        ref = b.at[r.same(r.left)]
        self.wire.go(self.key("left"), ref, ref, r.partner)
        self.wire.got(self.key("near", -1, 0))
        ref = b.at[r.same(r.right)]
        self.wire.go(self.key("right"), ref, ref, r.partner)

    def share_far(self):
        r, b = self.row, self.buf
        self.wire.got(self.key("far", 1))
        self.wire.got(self.key("far", -1))
        ref = b.at[r.same(r.across)]
        self.wire.go(self.key("across"), ref, ref, r.partner)

    def done(self):
        for k in ("own", "left", "right", "across"):
            self.wire.got(self.key(k))


class Sum:
    def __init__(self, wire, name, row, part, pair, stage, mid, end):
        self.wire, self.name, self.row = wire, name, row
        self.part, self.pair, self.stage, self.mid, self.end = part, pair, stage, mid, end

    def start(self):
        r = self.row
        self.wire.go((self.name, "pair"), self.part.at[1 - r.c], self.pair, r.partner)

    def both(self, x, half):
        rows = pl.ds(half * 128, 128)
        return f32(self.part[self.row.c, x, rows, :]) + f32(self.pair[x, rows, :])

    def out(self, k, value, dst, way):
        r = self.row
        self.stage[k] = value.astype(BF)
        self.wire.go((self.name, k), self.stage.at[k], dst, r.dev(r.right if way == 1 else r.left))

    def spread(self):
        r = self.row
        self.wire.got((self.name, "pair"))
        self.out(0, self.both(r.across, 0), self.mid.at[0], 1)
        self.out(1, self.both(r.across, 1), self.mid.at[1], -1)
        self.out(2, self.both(r.right, 1), self.end.at[0, 1], 1)
        self.out(3, self.both(r.left, 0), self.end.at[1, 0], -1)

    def relay(self):
        r = self.row
        self.wire.got((self.name, 0))
        self.out(4, self.both(r.right, 0) + f32(self.mid[0]), self.end.at[0, 0], 1)
        self.wire.got((self.name, 1))
        self.out(5, self.both(r.left, 1) + f32(self.mid[1]), self.end.at[1, 1], -1)

    def total(self, half):
        r = self.row
        if half == 0:
            for k in (2, 3, 4, 5):
                self.wire.got((self.name, k))
        return self.both(r.x, half) + f32(self.end[0, half]) + f32(self.end[1, half])


def normed_into(out, buf, gain):
    for half in (0, 1):
        for part in (0, 1):
            rows = pl.ds(part * 64, 64)
            sums = jnp.zeros((64, 256), F32)
            for j in range(N):
                v = f32(buf[j, half, rows, :])
                sums = sums + v * v
            mean = jnp.sum(sums, axis=1, keepdims=True) * (1.0 / (N * 256))
            factor = lax.rsqrt(mean + EPS)
            for j in range(N):
                v = f32(buf[j, half, rows, :])
                cols = pl.ds(j * 256, 256)
                out[pl.ds(half * 128 + part * 64, 64), cols] = (
                    v * factor * f32(gain[:, cols])
                ).astype(BF)


def kernel(
    tok,
    gain1,
    wb,
    wg,
    taps1,
    rmap,
    imap,
    rate,
    pld,
    wo,
    gain2,
    ug,
    uv,
    gtaps,
    vtaps,
    dn,
    out,
    gm,
    gu,
    gd,
    tokb,
    aftb,
    nrm,
    mixed,
    gv,
    hid,
    part1,
    pair1,
    stage1,
    mid1,
    end1,
    part2,
    pair2,
    stage2,
    mid2,
    end2,
    ssem,
    rsem,
):
    z, y, t = lax.axis_index("fs_0"), lax.axis_index("fs_1"), lax.axis_index("tp")
    here = (z, y, t)
    wire = Wire(ssem, rsem)
    row = Row(z, y, t)
    mix = Spread(wire, "mix", 0, gm, 2, here)
    up = Spread(wire, "up", 1, gu, 4, here)
    down = Spread(wire, "down", 2, gd, 2, here)
    ag1 = Gather(wire, "tok", tokb, row)
    ag2 = Gather(wire, "aft", aftb, row)
    rs1 = Sum(wire, "rs1", row, part1, pair1, stage1, mid1, end1)
    rs2 = Sum(wire, "rs2", row, part2, pair2, stage2, mid2, end2)

    barrier = pltpu.get_barrier_semaphore()
    peers = [
        mix.neighbour(0, 1),
        mix.neighbour(0, -1),
        mix.neighbour(1, 1),
        mix.neighbour(1, -1),
        row.dev(row.right),
        row.dev(row.left),
        row.partner,
    ]
    for peer in peers:
        pl.semaphore_signal(barrier, inc=1, device_id=peer, device_id_type=MESH)

    split = (2, 16)
    gm[z, y, :, :, 0:128] = wb[...].reshape(*split, 128)
    gm[z, y, :, :, 128:256] = wg[...].reshape(*split, 128)
    gm[z, y, :, :, 256:384] = wo[...].reshape(*split, 128)
    low, high = place(0), place(64)
    tokb[t] = tok[...].reshape(2, 128, 256)
    gu[z, y, :, :, 0:640] = ug[:, 0:640].reshape(*split, 640)
    gu[z, y, :, :, 640:1280] = uv[:, 0:640].reshape(*split, 640)
    tail = dot(ug[:, 640:704], low) + dot(uv[:, 640:704], high)
    gu[z, y, :, :, 1280:1408] = tail.astype(BF).reshape(*split, 128)
    gd[z, y, :, :, 0:640] = dn[:, 0:640].reshape(*split, 640)
    gd[z, y, :, :, 640:768] = dot(dn[:, 640:704], low).astype(BF).reshape(*split, 128)

    pl.semaphore_wait(barrier, len(peers))

    mix.send1(1)
    ag1.start()
    up.send1(1)
    down.send1(1)
    mix.forward1(1)
    up.forward1(1)
    mix.forward1(2)
    ag1.relay()
    down.forward1(1)
    mix.forward1(3)
    ag1.share()
    up.forward1(2)
    mix.forward1(4)
    mix.send2(0)
    mix.send2(1)
    ag1.share_far()
    up.forward1(3)
    down.forward1(2)
    up.forward1(4)
    up.send2(0)
    mix.forward2(0, 1)
    mix.forward2(1, 1)
    up.send2(1)
    down.forward1(3)
    ag1.done()
    normed_into(nrm, tokb, gain1)
    mix.forward2(0, 2)
    mix.forward2(1, 2)
    up.send2(2)
    up.forward2(0, 1)
    mix.forward2(0, 3)
    mix.forward2(1, 3)
    up.send2(3)
    up.forward2(1, 1)
    down.forward1(4)
    mix.forward2(0, 4)
    mix.forward2(1, 4)
    up.forward2(2, 1)

    both = dot(nrm[...], gm[:, :, :, :, 0:256].reshape(2048, 256))
    branch = both[:, 0:128].astype(BF)
    outgate = both[:, 128:256].astype(BF)
    up.forward2(0, 2)
    up.forward2(3, 1)
    rmat = jnp.concatenate([dot(rmap[0], low), dot(rmap[1], high)], axis=0).astype(BF)
    imat = jnp.concatenate([dot(imap[0], low), dot(imap[1], high)], axis=0).astype(BF)
    pos = lax.broadcasted_iota(jnp.int32, (SEQ, 128), 0)
    ctaps = f32(taps1[...])
    for s in range(4):
        rows = slice(s * SEQ, (s + 1) * SEQ)
        cv = conv(f32(branch[rows]), ctaps, pos).astype(BF)
        recur = jax.nn.sigmoid(dot(cv, rmat))
        inner = jax.nn.sigmoid(dot(cv, imat))
        loga = -DECAY_RATE_GAIN * recur * rate[...] + pld[rows, :]
        a = jnp.exp(loga)
        d = jnp.sqrt(jnp.tanh(-loga) * (1.0 + a * a)) * inner * f32(cv)
        k = 1
        while k < SEQ:
            d = d + a * shifted(d, k, pos)
            if 2 * k < SEQ:
                a = a * shifted(a, k, pos, 1.0)
            k *= 2
        mixed[rows, :] = (d * jax.nn.gelu(f32(outgate[rows]))).astype(BF)
    up.forward2(1, 2)
    for j in range(N):
        w = gm[j, :, :, :, 256:384].reshape(256, 128)
        part1[j % 2, j // 2] = dot_t(mixed[...], w).astype(BF)
    rs1.start()
    up.forward2(2, 2)
    rs1.spread()
    up.forward2(3, 2)
    down.send2(0)
    up.forward2(0, 3)
    rs1.relay()
    up.forward2(1, 3)
    for half in (0, 1):
        rows = pl.ds(half * 128, 128)
        aftb[t, half] = (f32(tok[rows, :]) + rs1.total(half)).astype(BF)
    ag2.start()
    up.forward2(2, 3)
    down.send2(1)
    ag2.relay()
    up.forward2(3, 3)
    ag2.share()
    down.forward2(0, 1)
    ag2.share_far()
    up.forward2(0, 4)
    up.forward2(1, 4)
    ag2.done()
    normed_into(nrm, aftb, gain2)
    down.forward2(1, 1)
    up.forward2(2, 4)
    up.forward2(3, 4)

    for k in range(6):
        cols = pl.ds(k * 256, 256 if k < 5 else 128)
        w = gu[:, :, :, :, cols]
        gv[:, cols] = dot(nrm[...], w.reshape(2048, w.shape[-1])).astype(BF)
        if k == 2:
            down.forward2(0, 2)
        if k == 4:
            down.forward2(1, 2)
    tail_taps = dot(gtaps[:, 640:704], low) + dot(vtaps[:, 640:704], high)
    lane = lax.broadcasted_iota(jnp.int32, (SEQ, 128), 1)
    for s in range(4):
        rows = pl.ds(s * SEQ, SEQ)
        for k in range(5):
            cols = pl.ds(k * 128, 128)
            g = conv(f32(gv[rows, cols]), f32(gtaps[:, cols]), pos)
            v = conv(f32(gv[rows, pl.ds(640 + k * 128, 128)]), f32(vtaps[:, cols]), pos)
            hid[rows, cols] = (jax.nn.silu(g) * v).astype(BF)
        b = conv(f32(gv[rows, pl.ds(1280, 128)]), tail_taps, pos)
        h = jnp.where(lane < 64, jax.nn.silu(b) * pltpu.roll(b, 64, 1), 0.0)
        hid[rows, pl.ds(640, 128)] = h.astype(BF)
    down.forward2(0, 3)
    down.forward2(1, 3)
    down.forward2(0, 4)
    down.forward2(1, 4)
    for j in range(N):
        w = gd[j].reshape(256, 768)
        part2[j % 2, j // 2] = dot_t(hid[...], w).astype(BF)
    rs2.start()
    rs2.spread()
    rs2.relay()
    for half in (0, 1):
        rows = pl.ds(half * 128, 128)
        out[rows, :] = (f32(aftb[t, half]) + rs2.total(half)).astype(BF)
    wire.finish()


def per_device(*args):
    (tok, gain1, wb, wg, taps1, rmap, imap, rate, pld, wo, gain2, ug, uv, gtaps, vtaps, dn) = args
    sums = [
        pltpu.VMEM((2, X, 256, 256), BF),
        pltpu.VMEM((X, 256, 256), BF),
        pltpu.VMEM((6, 128, 256), BF),
        pltpu.VMEM((2, 128, 256), BF),
        pltpu.VMEM((2, 2, 128, 256), BF),
    ]
    return pl.pallas_call(
        kernel,
        out_shape=jax.ShapeDtypeStruct((256, 256), BF),
        in_specs=[pl.BlockSpec(memory_space=pltpu.VMEM)] * 16,
        out_specs=pl.BlockSpec(memory_space=pltpu.VMEM),
        scratch_shapes=[
            pltpu.VMEM((N, N, 2, 16, 384), BF),
            pltpu.VMEM((N, N, 2, 16, 1408), BF),
            pltpu.VMEM((N, N, 2, 16, 768), BF),
            pltpu.VMEM((N, 2, 128, 256), BF),
            pltpu.VMEM((N, 2, 128, 256), BF),
            pltpu.VMEM((256, 2048), BF),
            pltpu.VMEM((256, 128), BF),
            pltpu.VMEM((256, 1408), BF),
            pltpu.VMEM((256, 768), BF),
            *sums,
            *sums,
            pltpu.SemaphoreType.DMA((MESSAGES,)),
            pltpu.SemaphoreType.DMA((MESSAGES,)),
        ],
        compiler_params=pltpu.CompilerParams(
            collective_id=0, has_side_effects=True, vmem_limit_bytes=48 * 2**20
        ),
        name="layer",
    )(
        tok,
        gain1.reshape(1, -1),
        wb,
        wg,
        taps1,
        rmap,
        imap,
        rate.reshape(1, -1),
        pld,
        wo.T,
        gain2.reshape(1, -1),
        ug,
        uv,
        gtaps,
        vtaps,
        dn.T,
    )


def solution(mesh):
    torus = Mesh(mesh.devices.reshape(N, N, mesh.shape["tp"]), ("fs_0", "fs_1", "tp"))
    return jax.shard_map(
        per_device,
        mesh=torus,
        in_specs=(
            P(FS, "tp"),
            P(),
            P(FS, "tp"),
            P(FS, "tp"),
            P(None, "tp"),
            P("tp", None, None),
            P("tp", None, None),
            P("tp"),
            P(FS, "tp"),
            P("tp", FS),
            P(),
            P(FS, "tp"),
            P(FS, "tp"),
            P(None, "tp"),
            P(None, "tp"),
            P("tp", FS),
        ),
        out_specs=P(FS, "tp"),
        check_vma=False,
    )
```

```python
import functools

import jax
import jax.numpy as jnp
from jax import lax
from jax.experimental import pallas as pl
from jax.experimental.pallas import tpu as pltpu
from jax.sharding import Mesh
from jax.sharding import PartitionSpec as P

SEQ = 64
FS = ("fs_0", "fs_1")
EPS = 1e-06
DECAY_RATE_GAIN = 8.0
BF = jnp.bfloat16
F32 = jnp.float32
MESH = pl.DeviceIdType.MESH
N = 8
X = 4
SENDS = 14
ARRIVALS = 100
CHUNKS = (4, 8, 4)
ORDER = (
    ("mix", "s1"),
    ("ag1", "start", 0),
    ("up", "s1"),
    ("up", "s2", 0),
    ("dn", "s1"),
    ("mix", "f1", 1),
    ("mix", "s2", 0),
    ("up", "f1", 1),
    ("up", "s2", 7),
    ("dn", "f1", 1),
    ("mix", "f1", 2),
    ("up", "s2", 1),
    ("up", "f2", 0, 1),
    ("up", "f1", 2),
    ("mix", "f2", 0, 1),
    ("ag1", "relay", 0),
    ("mix", "f1", 3),
    ("mix", "s2", 1),
    ("up", "s2", 2),
    ("mix", "s2", 3),
    ("dn", "f1", 2),
    ("up", "f2", 7, 1),
    ("mix", "f1", 4),
    ("mix", "s2", 2),
    ("mix", "f2", 1, 1),
    ("up", "f1", 3),
    ("dn", "s2", 0),
    ("mix", "f2", 3, 1),
    ("ag1", "share", 0),
    ("up", "f2", 2, 1),
    ("ag1", "sharefar", 0),
    ("mix", "f2", 2, 1),
    ("mix", "f2", 0, 2),
    ("up", "f2", 1, 1),
    ("mix", "f2", 1, 2),
    ("up", "s2", 3),
    ("up", "f2", 0, 2),
    ("mix", "f2", 2, 2),
    ("up", "f1", 4),
    ("mix", "f2", 3, 2),
    ("ag1", "done", 0),
    ("up", "s2", 4),
    ("dn", "f1", 3),
    ("up", "s2", 5),
    ("mix", "f2", 1, 3),
    ("norm1",),
    ("up", "s2", 6),
    ("mix", "f2", 0, 3),
    ("mix", "f2", 2, 3),
    ("mix", "f2", 3, 3),
    ("up", "f2", 4, 1),
    ("dn", "f1", 4),
    ("dn", "s2", 3),
    ("up", "f2", 3, 1),
    ("up", "f2", 1, 2),
    ("up", "f2", 5, 1),
    ("mix", "f2", 0, 4),
    ("mix", "f2", 3, 4),
    ("up", "f2", 7, 2),
    ("mix", "f2", 1, 4),
    ("up", "f2", 2, 2),
    ("up", "f2", 0, 3),
    ("mix", "f2", 2, 4),
    ("win",),
    ("mixer",),
    ("part1", 0),
    ("rs1", "start", 0),
    ("up", "f2", 6, 1),
    ("part1", 1),
    ("rs1", "start", 1),
    ("dn", "s2", 1),
    ("rs1", "spread", 0),
    ("up", "f2", 3, 2),
    ("dn", "s2", 2),
    ("up", "f2", 4, 2),
    ("rs1", "spread", 1),
    ("rs1", "relay", 0),
    ("up", "f2", 5, 2),
    ("rs1", "relay", 1),
    ("up", "f2", 6, 2),
    ("up", "f2", 7, 3),
    ("dn", "f2", 1, 1),
    ("rs1", "total", 0),
    ("up", "f2", 1, 3),
    ("ag2", "start", 0),
    ("up", "f2", 3, 3),
    ("dn", "f2", 0, 1),
    ("rs1", "total", 1),
    ("ag2", "start", 1),
    ("up", "f2", 4, 3),
    ("up", "f2", 5, 3),
    ("up", "f2", 6, 3),
    ("dn", "f2", 3, 1),
    ("up", "f2", 2, 3),
    ("dn", "f2", 2, 1),
    ("ag2", "relay", 0),
    ("ag2", "relay", 1),
    ("ag2", "share", 1),
    ("ag2", "share", 0),
    ("dn", "f2", 0, 2),
    ("up", "f2", 5, 4),
    ("ag2", "sharefar", 0),
    ("dn", "f2", 1, 2),
    ("dn", "f2", 3, 2),
    ("up", "f2", 1, 4),
    ("ag2", "sharefar", 1),
    ("up", "f2", 4, 4),
    ("up", "f2", 7, 4),
    ("up", "f2", 3, 4),
    ("up", "f2", 6, 4),
    ("up", "f2", 2, 4),
    ("dn", "f2", 2, 2),
    ("ag2", "done", 0),
    ("dn", "f2", 0, 3),
    ("ag2", "done", 1),
    ("norm2",),
    ("up", "f2", 0, 4),
    ("updot", 1),
    ("dn", "f2", 1, 3),
    ("updot", 3),
    ("dn", "f2", 3, 3),
    ("updot", 0),
    ("dn", "f2", 2, 3),
    ("updot", 5),
    ("updot", 2),
    ("updot", 4),
    ("dn", "f2", 1, 4),
    ("dn", "f2", 0, 4),
    ("hid",),
    ("dn", "f2", 3, 4),
    ("dn", "f2", 2, 4),
    ("part2",),
    ("rs2", "start", 0),
    ("rs2", "start", 1),
    ("rs2", "spread", 0),
    ("rs2", "spread", 1),
    ("rs2", "relay", 0),
    ("rs2", "relay", 1),
    ("rs2", "total", 0),
    ("rs2", "total", 1),
)
FIRST = (2, 3, 9, 0, 11, 12, 15)


def f32(v):
    return v.astype(F32)


def dot(a, b):
    return jnp.dot(a, b, preferred_element_type=F32)


def dot_t(a, b):
    return lax.dot_general(a, b, (((1,), (1,)), ((), ())), preferred_element_type=F32)


def place(offset):
    r = lax.broadcasted_iota(jnp.int32, (64, 128), 0)
    c = lax.broadcasted_iota(jnp.int32, (64, 128), 1)
    return jnp.where(c == r + offset, 1.0, 0.0).astype(BF)


def shifted(v, k, row, fill=0.0):
    return jnp.where(row >= k, pltpu.roll(v, k, 0), fill)


def conv(v, taps, row):
    width = taps.shape[0]
    total = v * taps[width - 1 : width]
    for k in range(1, width):
        total = total + shifted(v, k, row) * taps[width - 1 - k : width - k]
    return total


class Wire:
    def __init__(self, send, recv):
        self.send, self.recv, self.sent, self.due = send, recv, {}, {}

    def go(self, group, key, src, dst, dev):
        out = self.sent.setdefault(group, len(self.sent))
        into = self.due.setdefault(key, len(self.due))
        pltpu.make_async_remote_copy(
            src_ref=src,
            dst_ref=dst,
            send_sem=self.send.at[out],
            recv_sem=self.recv.at[into],
            device_id=dev,
            device_id_type=MESH,
        ).start()

    def got(self, key, ref):
        pltpu.make_async_copy(ref, ref, self.recv.at[self.due[key]]).wait()

    def gone(self, group, ref):
        pltpu.make_async_copy(ref, ref, self.send.at[self.sent[group]]).wait()


class Spread:
    def __init__(self, wire, name, index, buf, chunks, here):
        self.wire, self.name, self.index, self.buf, self.chunks = wire, name, index, buf, chunks
        self.z, self.y, self.t = here

    def neighbour(self, axis, way):
        if axis == 0:
            return (lax.rem(self.z + N + way, N), self.y, self.t)
        return (self.z, lax.rem(self.y + N + way, N), self.t)

    def first(self, half, way, step):
        axis = 1 - half
        pos = lax.rem((self.y if axis else self.z) + N - way * (step - 1), N)
        return self.buf.at[self.z, pos, 0] if half == 0 else self.buf.at[pos, self.y, 1]

    def pass1(self, step):
        for half in (0, 1):
            for way in (1, -1):
                far = 1 if (self.index + half) % 2 == 0 else -1
                if step < N // 2 or (step == N // 2 and way == far):
                    ref = self.first(half, way, step)
                    dev = self.neighbour(1 - half, way)
                    self.wire.go(self.name, (self.name, step), ref, ref, dev)

    def forward1(self, step):
        self.wire.got((self.name, step), self.buf.at[0, pl.ds(0, 2 if step < N // 2 else 1)])
        self.pass1(step + 1)

    def second(self, half, way, step, q):
        size = N // self.chunks
        own = (self.z if half else self.y) // size
        part = pl.ds(lax.rem(own + q, self.chunks) * size, size)
        pos = lax.rem((self.y if half else self.z) + N - way * (step - 1), N)
        return self.buf.at[pos, part, 0] if half == 0 else self.buf.at[part, pos, 1]

    def pass2(self, q, step):
        far = 1 if q < self.chunks // 2 else -1
        for half in (0, 1):
            for way in (1, -1):
                if step < N // 2 or (step == N // 2 and way == far):
                    ref = self.second(half, way, step, q)
                    dev = self.neighbour(half, way)
                    self.wire.go(self.name, (self.name, step, q), ref, ref, dev)

    def forward2(self, q, step):
        size = N // self.chunks
        self.wire.got(
            (self.name, step, q), self.buf.at[0, pl.ds(0, 2 * size if step < N // 2 else size)]
        )
        self.pass2(q, step + 1)

    def finish(self):
        self.wire.gone(self.name, self.buf.reshape(N * N, *self.buf.shape[2:]).at[pl.ds(0, N * N - 1)])


class Row:
    def __init__(self, z, y, t):
        self.z, self.y, self.t = z, y, t
        self.x, self.c = t // 2, lax.rem(t, 2)
        self.right = lax.rem(self.x + 1, X)
        self.left = lax.rem(self.x + X - 1, X)
        self.across = lax.rem(self.x + 2, X)

    def dev(self, x):
        return (self.z, self.y, 2 * x + self.c)

    def same(self, x):
        return 2 * x + self.c

    @property
    def partner(self):
        return (self.z, self.y, 2 * self.x + 1 - self.c)


class Gather:
    def __init__(self, wire, name, buf, row):
        self.wire, self.name, self.buf, self.row = wire, name, buf, row

    def go(self, key, ref, dev):
        self.wire.go(self.name, (self.name, key), ref, ref, dev)

    def got(self, key, count):
        self.wire.got((self.name, key), self.buf.at[pl.ds(0, count)])

    def start(self):
        r, b = self.row, self.buf
        for k in (0, 1):
            self.go(k, b.at[r.t, k], r.dev(r.right))
            self.go(k, b.at[r.t, 1 - k], r.dev(r.left))
        self.go("pair", b.at[r.t], r.partner)

    def relay(self):
        r, b = self.row, self.buf
        self.got(0, 1)
        self.go("far", b.at[r.same(r.left), 0], r.dev(r.right))
        self.go("far", b.at[r.same(r.right), 1], r.dev(r.left))

    def share(self):
        r, b = self.row, self.buf
        self.got(1, 1)
        self.go("pair", b.at[r.same(r.left)], r.partner)
        self.go("pair", b.at[r.same(r.right)], r.partner)

    def share_far(self):
        r, b = self.row, self.buf
        self.got("far", 1)
        self.go("pair", b.at[r.same(r.across)], r.partner)

    def done(self):
        self.got("pair", 4)

    def finish(self):
        self.wire.gone(self.name, self.buf.at[pl.ds(0, 7)])


class Sum:
    def __init__(self, wire, name, row, part, pair, stage, mid, end):
        self.wire, self.name, self.row = wire, name, row
        self.part, self.pair, self.stage, self.mid, self.end = part, pair, stage, mid, end

    def key(self, k):
        return (self.name, k)

    def start(self):
        r = self.row
        self.wire.go(self.key(0), self.key(0), self.part.at[1 - r.c], self.pair, r.partner)

    def both(self, x, half):
        rows = pl.ds(half * 128, 128)
        return f32(self.part[self.row.c, x, rows, :]) + f32(self.pair[x, rows, :])

    def out(self, k, value, dst, way):
        r = self.row
        self.stage[k] = value.astype(BF)
        dev = r.dev(r.right if way == 1 else r.left)
        self.wire.go(self.key(1), self.key(1 if k < 2 else 2), self.stage.at[k], dst, dev)

    def spread(self):
        r = self.row
        self.wire.got(self.key(0), self.pair)
        self.out(0, self.both(r.across, 0), self.mid.at[0], 1)
        self.out(1, self.both(r.across, 1), self.mid.at[1], -1)
        self.out(2, self.both(r.right, 1), self.end.at[0, 1], 1)
        self.out(3, self.both(r.left, 0), self.end.at[1, 0], -1)

    def relay(self):
        r = self.row
        self.wire.got(self.key(1), self.mid)
        self.out(4, self.both(r.right, 0) + f32(self.mid[0]), self.end.at[0, 0], 1)
        self.out(5, self.both(r.left, 1) + f32(self.mid[1]), self.end.at[1, 1], -1)

    def total(self, half):
        r = self.row
        if half == 0:
            self.wire.got(self.key(2), self.end)
        return self.both(r.x, half) + f32(self.end[0, half]) + f32(self.end[1, half])

    def finish(self):
        self.wire.gone(self.key(0), self.pair)
        self.wire.gone(self.key(1), self.stage)


def normed_into(out, bufs, gain):
    width = 256 // len(bufs)
    for half in (0, 1):
        for part in (0, 1):
            rows = pl.ds(part * 64, 64)
            sums = jnp.zeros((64, width), F32)
            for j in range(N):
                for buf in bufs:
                    v = f32(buf[j, half, rows, :])
                    sums = sums + v * v
            mean = jnp.sum(sums, axis=1, keepdims=True) * (1.0 / (N * 256))
            factor = lax.rsqrt(mean + EPS)
            for j in range(N):
                for k, buf in enumerate(bufs):
                    v = f32(buf[j, half, rows, :])
                    cols = pl.ds(j * 256 + k * width, width)
                    scale = f32(gain[cols].reshape(1, width))
                    out[pl.ds(half * 128 + part * 64, 64), cols] = (v * factor * scale).astype(BF)


def kernel(*refs):
    sources, refs = refs[:16], refs[16:]
    out, staged, in_sem, refs = refs[0], refs[1:17], refs[17], refs[18:]
    fetch = [
        pltpu.make_async_copy(source, target, in_sem.at[k])
        for k, (source, target) in enumerate(zip(sources, staged))
    ]
    for k in FIRST:
        fetch[k].start()
    for k in range(16):
        if k not in FIRST:
            fetch[k].start()
    body(fetch, out, *staged, *refs)


def body(
    fetch,
    out,
    tok,
    gain1,
    wb,
    wg,
    taps1,
    rmap,
    imap,
    rate,
    pld,
    wo,
    gain2,
    ug,
    uv,
    gtaps,
    vtaps,
    dn,
    gm,
    gu,
    gd,
    tokb,
    aftb,
    nrm,
    pair,
    mixed,
    gv,
    hid,
    part1,
    pair1,
    stage1,
    mid1,
    end1,
    part2,
    pair2,
    stage2,
    mid2,
    end2,
    ssem,
    rsem,
):
    z, y, t = lax.axis_index("fs_0"), lax.axis_index("fs_1"), lax.axis_index("tp")
    here = (z, y, t)
    wire = Wire(ssem, rsem)
    row = Row(z, y, t)
    mix = Spread(wire, "mix", 0, gm, CHUNKS[0], here)
    up = Spread(wire, "up", 1, gu, CHUNKS[1], here)
    down = Spread(wire, "dn", 2, gd, CHUNKS[2], here)
    ag1 = Gather(wire, "tok", tokb, row)
    ag2 = [Gather(wire, ("aft", k), aftb.at[k], row) for k in (0, 1)]
    rs1, rs2 = (
        [Sum(wire, (name, k), row, *(ref.at[k] for ref in refs)) for k in (0, 1)]
        for name, refs in (
            ("rs1", (part1, pair1, stage1, mid1, end1)),
            ("rs2", (part2, pair2, stage2, mid2, end2)),
        )
    )

    barrier = pltpu.get_barrier_semaphore()
    peers = [
        mix.neighbour(0, 1),
        mix.neighbour(0, -1),
        mix.neighbour(1, 1),
        mix.neighbour(1, -1),
        row.dev(row.right),
        row.dev(row.left),
        row.partner,
    ]
    for peer in peers:
        pl.semaphore_signal(barrier, inc=1, device_id=peer, device_id_type=MESH)

    split = (2, 16)
    for k in FIRST:
        fetch[k].wait()
    gm[z, y, :, :, 0:128] = wb[...].reshape(*split, 128)
    gm[z, y, :, :, 128:256] = wg[...].reshape(*split, 128)
    gm[z, y, :, :, 256:384] = wo[...].reshape(*split, 128)
    low, high = place(0), place(64)
    tokb[t] = tok[...].reshape(2, 128, 256)
    gu[z, y, :, :, 0:640] = ug[:, 0:640].reshape(*split, 640)
    gu[z, y, :, :, 640:1280] = uv[:, 0:640].reshape(*split, 640)
    tail = dot(ug[:, 640:704], low) + dot(uv[:, 640:704], high)
    gu[z, y, :, :, 1280:1408] = tail.astype(BF).reshape(*split, 128)
    gd[z, y, :, :, 0:640] = dn[:, 0:640].reshape(*split, 640)
    gd[z, y, :, :, 640:768] = dot(dn[:, 640:704], low).astype(BF).reshape(*split, 128)

    pl.semaphore_wait(barrier, len(peers))
    for k in range(16):
        if k not in FIRST:
            fetch[k].wait()

    pos = lax.broadcasted_iota(jnp.int32, (SEQ, 128), 0)
    lane = lax.broadcasted_iota(jnp.int32, (SEQ, 128), 1)

    def project():
        w = gm[:, :, :, :, 0:256].reshape(2048, 256)
        pair[...] = dot(nrm[...], w).astype(BF)

    def recurrence():
        rmat = jnp.concatenate([dot(rmap[0], low), dot(rmap[1], high)], axis=0).astype(BF)
        imat = jnp.concatenate([dot(imap[0], low), dot(imap[1], high)], axis=0).astype(BF)
        for s in range(4):
            rows = slice(s * SEQ, (s + 1) * SEQ)
            cv = conv(f32(pair[rows, 0:128]), f32(taps1[...]), pos).astype(BF)
            recur = jax.nn.sigmoid(dot(cv, rmat))
            inner = jax.nn.sigmoid(dot(cv, imat))
            loga = -DECAY_RATE_GAIN * recur * rate[...].reshape(1, 128) + pld[rows, :]
            a = jnp.exp(loga)
            d = jnp.sqrt(jnp.tanh(-loga) * (1.0 + a * a)) * inner * f32(cv)
            k = 1
            while k < SEQ:
                d = d + a * shifted(d, k, pos)
                if 2 * k < SEQ:
                    a = a * shifted(a, k, pos, 1.0)
                k *= 2
            mixed[rows, :] = (d * jax.nn.gelu(f32(pair[rows, 128:256]))).astype(BF)

    def mixer_out(k):
        for j in range(N):
            w = gm[j, 4 * k : 4 * k + 4, :, :, 256:384].reshape(128, 128)
            part1[k, j % 2, j // 2] = dot_t(mixed[...], w).astype(BF)

    def residual(k):
        cols = pl.ds(k * 128, 128)
        for half in (0, 1):
            rows = pl.ds(half * 128, 128)
            aftb[k, t, half] = (f32(tok[rows, cols]) + rs1[k].total(half)).astype(BF)

    def expand(k):
        cols = pl.ds(k * 256, 256 if k < 5 else 128)
        w = gu[:, :, :, :, cols]
        gv[:, cols] = dot(nrm[...], w.reshape(2048, w.shape[-1])).astype(BF)

    def gated():
        tail_taps = dot(gtaps[:, 640:704], low) + dot(vtaps[:, 640:704], high)
        for s in range(4):
            rows = pl.ds(s * SEQ, SEQ)
            for k in range(5):
                cols = pl.ds(k * 128, 128)
                g = conv(f32(gv[rows, cols]), f32(gtaps[:, cols]), pos)
                v = conv(f32(gv[rows, pl.ds(640 + k * 128, 128)]), f32(vtaps[:, cols]), pos)
                hid[rows, cols] = (jax.nn.silu(g) * v).astype(BF)
            b = conv(f32(gv[rows, pl.ds(1280, 128)]), tail_taps, pos)
            h = jnp.where(lane < 64, jax.nn.silu(b) * pltpu.roll(b, 64, 1), 0.0)
            hid[rows, pl.ds(640, 128)] = h.astype(BF)

    def contract():
        for j in range(N):
            sums = dot_t(hid[...], gd[j].reshape(256, 768)).astype(BF)
            for k in (0, 1):
                part2[k, j % 2, j // 2] = sums[:, k * 128 : k * 128 + 128]

    def result(k):
        cols = pl.ds(k * 128, 128)
        for half in (0, 1):
            rows = pl.ds(half * 128, 128)
            out[rows, cols] = (f32(aftb[k, t, half]) + rs2[k].total(half)).astype(BF)

    spreads = {"mix": mix, "up": up, "dn": down}
    steps = {
        ("norm1",): lambda: normed_into(nrm, (tokb,), gain1),
        ("win",): project,
        ("mixer",): recurrence,
        ("norm2",): lambda: normed_into(nrm, (aftb.at[0], aftb.at[1]), gain2),
        ("hid",): gated,
        ("part2",): contract,
    }
    for k in (0, 1):
        steps["part1", k] = functools.partial(mixer_out, k)
        steps["rs1", "total", k] = functools.partial(residual, k)
        steps["rs2", "total", k] = functools.partial(result, k)
    for name, k, gather in (("ag1", 0, ag1), ("ag2", 0, ag2[0]), ("ag2", 1, ag2[1])):
        steps[name, "start", k] = gather.start
        steps[name, "relay", k] = gather.relay
        steps[name, "share", k] = gather.share
        steps[name, "sharefar", k] = gather.share_far
        steps[name, "done", k] = gather.done
    for name, parts in (("rs1", rs1), ("rs2", rs2)):
        for k in (0, 1):
            steps[name, "start", k] = parts[k].start
            steps[name, "spread", k] = parts[k].spread
            steps[name, "relay", k] = parts[k].relay
    for step in ORDER:
        if step[0] in spreads:
            spread, what, rest = spreads[step[0]], step[1], step[2:]
            if what == "s1":
                spread.pass1(1)
            elif what == "f1":
                spread.forward1(*rest)
            elif what == "s2":
                spread.pass2(*rest, 1)
            else:
                spread.forward2(*rest)
        elif step[0] == "updot":
            expand(step[1])
        else:
            steps[step]()
    for part in (mix, up, down, ag1, *ag2, *rs1, *rs2):
        part.finish()


def per_device(*args):
    (tok, gain1, wb, wg, taps1, rmap, imap, rate, pld, wo, gain2, ug, uv, gtaps, vtaps, dn) = args
    sums = [
        pltpu.VMEM((2, 2, X, 256, 128), BF),
        pltpu.VMEM((2, X, 256, 128), BF),
        pltpu.VMEM((2, 6, 128, 128), BF),
        pltpu.VMEM((2, 2, 128, 128), BF),
        pltpu.VMEM((2, 2, 2, 128, 128), BF),
    ]
    operands = (
        tok, gain1, wb, wg, taps1, rmap, imap, rate, pld, wo.T, gain2, ug, uv, gtaps, vtaps, dn.T
    )
    return pl.pallas_call(
        kernel,
        out_shape=jax.ShapeDtypeStruct((256, 256), BF),
        in_specs=[pl.BlockSpec(memory_space=pltpu.HBM)] * 16,
        out_specs=pl.BlockSpec(memory_space=pltpu.VMEM),
        scratch_shapes=[
            *[pltpu.VMEM(a.shape, a.dtype) for a in operands],
            pltpu.SemaphoreType.DMA((16,)),
            pltpu.VMEM((N, N, 2, 16, 384), BF),
            pltpu.VMEM((N, N, 2, 16, 1408), BF),
            pltpu.VMEM((N, N, 2, 16, 768), BF),
            pltpu.VMEM((N, 2, 128, 256), BF),
            pltpu.VMEM((2, N, 2, 128, 128), BF),
            pltpu.VMEM((256, 2048), BF),
            pltpu.VMEM((256, 256), BF),
            pltpu.VMEM((256, 128), BF),
            pltpu.VMEM((256, 1408), BF),
            pltpu.VMEM((256, 768), BF),
            *sums,
            *sums,
            pltpu.SemaphoreType.DMA((SENDS,)),
            pltpu.SemaphoreType.DMA((ARRIVALS,)),
        ],
        compiler_params=pltpu.CompilerParams(
            collective_id=0, has_side_effects=True, vmem_limit_bytes=67043328
        ),
        name="layer",
    )(*operands)


def solution(mesh):
    torus = Mesh(mesh.devices.reshape(N, N, mesh.shape["tp"]), ("fs_0", "fs_1", "tp"))
    return jax.shard_map(
        per_device,
        mesh=torus,
        in_specs=(
            P(FS, "tp"),
            P(),
            P(FS, "tp"),
            P(FS, "tp"),
            P(None, "tp"),
            P("tp", None, None),
            P("tp", None, None),
            P("tp"),
            P(FS, "tp"),
            P("tp", FS),
            P(),
            P(FS, "tp"),
            P(FS, "tp"),
            P(None, "tp"),
            P(None, "tp"),
            P("tp", FS),
        ),
        out_specs=P(FS, "tp"),
        check_vma=False,
    )
```

```python
import functools

import jax
import jax.numpy as jnp
from jax import lax
from jax.experimental import pallas as pl
from jax.experimental.pallas import tpu as pltpu
from jax.sharding import Mesh
from jax.sharding import PartitionSpec as P

SEQ = 64
FS = ("fs_0", "fs_1")
EPS = 1e-06
DECAY_RATE_GAIN = 8.0
BF = jnp.bfloat16
F32 = jnp.float32
MESH = pl.DeviceIdType.MESH
N = 8
X = 4
MIX, UP, DN, AG1, AG2, RS1, RS2 = range(7)
NORM1, WIN, MIXER, PART1, NORM2, UPDOT, HID, PART2 = range(7, 15)
S1, F1, S2, F2, START, RELAY, SHARE, SHAREFAR, DONE, SPREAD, REST, TOTAL = range(12)
SENDS = 14
ARRIVALS = 120
CHUNKS = (4, 8, 8)
ORDER = (
    (MIX, S1),
    (DN, S1),
    (UP, S1),
    (DN, S2, 0),
    (UP, S2, 0),
    (MIX, F1, 1),
    (MIX, S2, 0),
    (DN, F1, 1),
    (DN, S2, 7),
    (UP, F1, 1),
    (DN, S2, 1),
    (UP, S2, 1),
    (AG1, START, 0),
    (MIX, F1, 2),
    (UP, S2, 7),
    (UP, F2, 0, 1),
    (MIX, F2, 0, 1),
    (UP, F1, 2),
    (MIX, F1, 3),
    (AG1, RELAY, 0),
    (AG1, SHARE, 0),
    (MIX, S2, 3),
    (MIX, S2, 1),
    (UP, S2, 2),
    (UP, F2, 1, 1),
    (DN, F1, 2),
    (MIX, F1, 4),
    (MIX, S2, 2),
    (UP, F1, 3),
    (MIX, F2, 1, 1),
    (AG1, SHAREFAR, 0),
    (MIX, F2, 3, 1),
    (UP, F2, 7, 1),
    (DN, S2, 2),
    (AG1, DONE, 0),
    (MIX, F2, 0, 2),
    (MIX, F2, 2, 1),
    (UP, S2, 5),
    (UP, F1, 4),
    (MIX, F2, 1, 2),
    (MIX, F2, 3, 2),
    (UP, S2, 4),
    (MIX, F2, 0, 3),
    (MIX, F2, 2, 2),
    (UP, S2, 3),
    (UP, F2, 5, 1),
    (MIX, F2, 1, 3),
    (UP, F2, 2, 1),
    (MIX, F2, 3, 3),
    (DN, F1, 3),
    (MIX, F2, 2, 3),
    (DN, S2, 5),
    (DN, S2, 6),
    (UP, S2, 6),
    (UP, F2, 3, 1),
    (UP, F2, 4, 1),
    (UP, F2, 1, 2),
    (DN, F2, 7, 1),
    (NORM1,),
    (MIX, F2, 1, 4),
    (UP, F2, 7, 2),
    (MIX, F2, 0, 4),
    (DN, S2, 3),
    (MIX, F2, 3, 4),
    (MIX, F2, 2, 4),
    (WIN,),
    (MIXER,),
    (PART1, 1),
    (RS1, START, 1),
    (PART1, 0),
    (RS1, START, 0),
    (RS1, SPREAD, 1),
    (UP, F2, 6, 1),
    (UP, F2, 5, 2),
    (RS1, SPREAD, 0),
    (UP, F2, 2, 2),
    (RS1, REST, 1),
    (DN, F1, 4),
    (RS1, REST, 0),
    (DN, F2, 5, 1),
    (UP, F2, 3, 2),
    (DN, F2, 2, 1),
    (RS1, RELAY, 1),
    (DN, F2, 3, 1),
    (UP, F2, 0, 2),
    (DN, S2, 4),
    (RS1, RELAY, 0),
    (UP, F2, 4, 2),
    (UP, F2, 6, 2),
    (RS1, TOTAL, 1),
    (AG2, START, 1),
    (UP, F2, 1, 3),
    (DN, F2, 6, 1),
    (UP, F2, 7, 3),
    (DN, F2, 0, 1),
    (DN, F2, 1, 1),
    (RS1, TOTAL, 0),
    (AG2, START, 0),
    (UP, F2, 5, 3),
    (AG2, RELAY, 1),
    (UP, F2, 3, 3),
    (UP, F2, 2, 3),
    (UP, F2, 6, 3),
    (UP, F2, 0, 3),
    (AG2, SHARE, 1),
    (AG2, RELAY, 0),
    (UP, F2, 4, 3),
    (DN, F2, 4, 1),
    (DN, F2, 7, 2),
    (DN, F2, 2, 2),
    (DN, F2, 1, 2),
    (UP, F2, 7, 4),
    (AG2, SHAREFAR, 1),
    (DN, F2, 6, 2),
    (AG2, SHARE, 0),
    (DN, F2, 3, 2),
    (DN, F2, 0, 2),
    (DN, F2, 5, 2),
    (AG2, SHAREFAR, 0),
    (UP, F2, 1, 4),
    (UP, F2, 6, 4),
    (AG2, DONE, 1),
    (UP, F2, 0, 4),
    (UP, F2, 2, 4),
    (DN, F2, 4, 2),
    (UP, F2, 3, 4),
    (UP, F2, 5, 4),
    (UP, F2, 4, 4),
    (AG2, DONE, 0),
    (NORM2,),
    (UPDOT, 0),
    (DN, F2, 2, 3),
    (DN, F2, 7, 3),
    (UPDOT, 4),
    (DN, F2, 1, 3),
    (DN, F2, 6, 3),
    (DN, F2, 3, 3),
    (UPDOT, 5),
    (DN, F2, 0, 3),
    (DN, F2, 5, 3),
    (UPDOT, 2),
    (DN, F2, 4, 3),
    (UPDOT, 1),
    (UPDOT, 3),
    (DN, F2, 2, 4),
    (HID,),
    (DN, F2, 1, 4),
    (DN, F2, 7, 4),
    (DN, F2, 6, 4),
    (DN, F2, 0, 4),
    (DN, F2, 3, 4),
    (DN, F2, 5, 4),
    (PART2, 0),
    (DN, F2, 4, 4),
    (PART2, 1),
    (RS2, START, 0),
    (RS2, START, 1),
    (RS2, SPREAD, 0),
    (RS2, SPREAD, 1),
    (RS2, REST, 0),
    (RS2, REST, 1),
    (RS2, RELAY, 0),
    (RS2, RELAY, 1),
    (RS2, TOTAL, 0),
    (RS2, TOTAL, 1),
)
FIRST = (2, 3, 9, 0, 11, 12, 15)


def f32(v):
    return v.astype(F32)


def dot(a, b):
    return jnp.dot(a, b, preferred_element_type=F32)


def dot_t(a, b):
    return lax.dot_general(a, b, (((1,), (1,)), ((), ())), preferred_element_type=F32)


def place(offset):
    r = lax.broadcasted_iota(jnp.int32, (64, 128), 0)
    c = lax.broadcasted_iota(jnp.int32, (64, 128), 1)
    return jnp.where(c == r + offset, 1.0, 0.0).astype(BF)


def shifted(v, k, row, fill=0.0):
    return jnp.where(row >= k, pltpu.roll(v, k, 0), fill)


def conv(v, taps, row):
    width = taps.shape[0]
    total = v * taps[width - 1 : width]
    for k in range(1, width):
        total = total + shifted(v, k, row) * taps[width - 1 - k : width - k]
    return total


class Wire:
    def __init__(self, send, recv):
        self.send, self.recv, self.sent, self.due = send, recv, {}, {}

    def go(self, group, key, src, dst, dev):
        out = self.sent.setdefault(group, len(self.sent))
        into = self.due.setdefault(key, len(self.due))
        pltpu.make_async_remote_copy(
            src_ref=src,
            dst_ref=dst,
            send_sem=self.send.at[out],
            recv_sem=self.recv.at[into],
            device_id=dev,
            device_id_type=MESH,
        ).start()

    def got(self, key, ref):
        pltpu.make_async_copy(ref, ref, self.recv.at[self.due[key]]).wait()

    def gone(self, group, ref):
        pltpu.make_async_copy(ref, ref, self.send.at[self.sent[group]]).wait()


class Spread:
    def __init__(self, wire, name, index, buf, chunks, here):
        self.wire, self.name, self.index, self.buf, self.chunks = wire, name, index, buf, chunks
        self.z, self.y, self.t = here

    def neighbour(self, axis, way):
        if axis == 0:
            return (lax.rem(self.z + N + way, N), self.y, self.t)
        return (self.z, lax.rem(self.y + N + way, N), self.t)

    def first(self, half, way, step):
        axis = 1 - half
        pos = lax.rem((self.y if axis else self.z) + N - way * (step - 1), N)
        return self.buf.at[self.z, pos, 0] if half == 0 else self.buf.at[pos, self.y, 1]

    def pass1(self, step):
        for half in (0, 1):
            for way in (1, -1):
                far = 1 if (self.index + half) % 2 == 0 else -1
                if step < N // 2 or (step == N // 2 and way == far):
                    ref = self.first(half, way, step)
                    dev = self.neighbour(1 - half, way)
                    self.wire.go(self.name, (self.name, step), ref, ref, dev)

    def forward1(self, step):
        self.wire.got((self.name, step), self.buf.at[0, pl.ds(0, 2 if step < N // 2 else 1)])
        self.pass1(step + 1)

    def second(self, half, way, step, q):
        size = N // self.chunks
        own = (self.z if half else self.y) // size
        part = pl.ds(lax.rem(own + q, self.chunks) * size, size)
        pos = lax.rem((self.y if half else self.z) + N - way * (step - 1), N)
        return self.buf.at[pos, part, 0] if half == 0 else self.buf.at[part, pos, 1]

    def pass2(self, q, step):
        far = 1 if q < self.chunks // 2 else -1
        for half in (0, 1):
            for way in (1, -1):
                if step < N // 2 or (step == N // 2 and way == far):
                    ref = self.second(half, way, step, q)
                    dev = self.neighbour(half, way)
                    self.wire.go(self.name, (self.name, step, q), ref, ref, dev)

    def forward2(self, q, step):
        size = N // self.chunks
        self.wire.got(
            (self.name, step, q), self.buf.at[0, pl.ds(0, 2 * size if step < N // 2 else size)]
        )
        self.pass2(q, step + 1)

    def finish(self):
        self.wire.gone(self.name, self.buf.reshape(N * N, *self.buf.shape[2:]).at[pl.ds(0, N * N - 1)])


class Row:
    def __init__(self, z, y, t):
        self.z, self.y, self.t = z, y, t
        self.x, self.c = t // 2, lax.rem(t, 2)
        self.right = lax.rem(self.x + 1, X)
        self.left = lax.rem(self.x + X - 1, X)
        self.across = lax.rem(self.x + 2, X)

    def dev(self, x):
        return (self.z, self.y, 2 * x + self.c)

    def same(self, x):
        return 2 * x + self.c

    @property
    def partner(self):
        return (self.z, self.y, 2 * self.x + 1 - self.c)


class Gather:
    def __init__(self, wire, name, buf, row):
        self.wire, self.name, self.buf, self.row = wire, name, buf, row

    def go(self, key, ref, dev):
        self.wire.go(self.name, (self.name, key), ref, ref, dev)

    def got(self, key, count):
        self.wire.got((self.name, key), self.buf.at[pl.ds(0, count)])

    def start(self):
        r, b = self.row, self.buf
        for k in (0, 1):
            self.go(k, b.at[r.t, k], r.dev(r.right))
            self.go(k, b.at[r.t, 1 - k], r.dev(r.left))
        self.go("pair", b.at[r.t], r.partner)

    def relay(self):
        r, b = self.row, self.buf
        self.got(0, 1)
        self.go("far", b.at[r.same(r.left), 0], r.dev(r.right))
        self.go("far", b.at[r.same(r.right), 1], r.dev(r.left))

    def share(self):
        r, b = self.row, self.buf
        self.got(1, 1)
        self.go("pair", b.at[r.same(r.left)], r.partner)
        self.go("pair", b.at[r.same(r.right)], r.partner)

    def share_far(self):
        r, b = self.row, self.buf
        self.got("far", 1)
        self.go("pair", b.at[r.same(r.across)], r.partner)

    def done(self):
        self.got("pair", 4)

    def finish(self):
        self.wire.gone(self.name, self.buf.at[pl.ds(0, 7)])


class Sum:
    def __init__(self, wire, name, row, part, pair, stage, mid, end):
        self.wire, self.name, self.row = wire, name, row
        self.part, self.pair, self.stage, self.mid, self.end = part, pair, stage, mid, end

    def key(self, k):
        return (self.name, k)

    def start(self):
        r = self.row
        for x, key in ((r.across, 0), (r.right, 3), (r.left, 3), (r.x, 3)):
            src, dst = self.part.at[1 - r.c, x], self.pair.at[x]
            self.wire.go(self.key(0), self.key(key), src, dst, r.partner)

    def both(self, x, half):
        rows = pl.ds(half * 128, 128)
        return f32(self.part[self.row.c, x, rows, :]) + f32(self.pair[x, rows, :])

    def out(self, k, value, dst, way):
        r = self.row
        self.stage[k] = value.astype(BF)
        dev = r.dev(r.right if way == 1 else r.left)
        self.wire.go(self.key(1), self.key(1 if k < 2 else 2), self.stage.at[k], dst, dev)

    def spread(self):
        r = self.row
        self.wire.got(self.key(0), self.pair.at[0])
        self.out(0, self.both(r.across, 0), self.mid.at[0], 1)
        self.out(1, self.both(r.across, 1), self.mid.at[1], -1)

    def rest(self):
        r = self.row
        self.wire.got(self.key(3), self.pair.at[pl.ds(0, 3)])
        self.out(2, self.both(r.right, 1), self.end.at[0, 1], 1)
        self.out(3, self.both(r.left, 0), self.end.at[1, 0], -1)

    def relay(self):
        r = self.row
        self.wire.got(self.key(1), self.mid)
        self.out(4, self.both(r.right, 0) + f32(self.mid[0]), self.end.at[0, 0], 1)
        self.out(5, self.both(r.left, 1) + f32(self.mid[1]), self.end.at[1, 1], -1)

    def total(self, half):
        r = self.row
        if half == 0:
            self.wire.got(self.key(2), self.end)
        return self.both(r.x, half) + f32(self.end[0, half]) + f32(self.end[1, half])

    def finish(self):
        self.wire.gone(self.key(0), self.pair)
        self.wire.gone(self.key(1), self.stage)


def normed_into(out, bufs, gain):
    width = 256 // len(bufs)
    for half in (0, 1):
        for part in (0, 1):
            rows = pl.ds(part * 64, 64)
            sums = jnp.zeros((64, width), F32)
            for j in range(N):
                for buf in bufs:
                    v = f32(buf[j, half, rows, :])
                    sums = sums + v * v
            mean = jnp.sum(sums, axis=1, keepdims=True) * (1.0 / (N * 256))
            factor = lax.rsqrt(mean + EPS)
            for j in range(N):
                for k, buf in enumerate(bufs):
                    v = f32(buf[j, half, rows, :])
                    cols = pl.ds(j * 256 + k * width, width)
                    scale = f32(gain[cols].reshape(1, width))
                    out[pl.ds(half * 128 + part * 64, 64), cols] = (v * factor * scale).astype(BF)


def kernel(*refs):
    sources, refs = refs[:16], refs[16:]
    out, staged, in_sem, refs = refs[0], refs[1:17], refs[17], refs[18:]
    fetch = [
        pltpu.make_async_copy(source, target, in_sem.at[k])
        for k, (source, target) in enumerate(zip(sources, staged))
    ]
    for k in FIRST:
        fetch[k].start()
    for k in range(16):
        if k not in FIRST:
            fetch[k].start()
    body(fetch, in_sem, out, *staged, *refs)


def body(
    fetch,
    in_sem,
    out,
    tok,
    gain1,
    wb,
    wg,
    taps1,
    rmap,
    imap,
    rate,
    pld,
    wo,
    gain2,
    ug,
    uv,
    gtaps,
    vtaps,
    dn,
    gm,
    gu,
    gd,
    tokb,
    aftb,
    nrm,
    pair,
    mixed,
    gv,
    hid,
    part1,
    pair1,
    stage1,
    mid1,
    end1,
    part2,
    pair2,
    stage2,
    mid2,
    end2,
    final,
    ssem,
    rsem,
):
    z, y, t = lax.axis_index("fs_0"), lax.axis_index("fs_1"), lax.axis_index("tp")
    here = (z, y, t)
    wire = Wire(ssem, rsem)
    row = Row(z, y, t)
    mix = Spread(wire, "mix", 0, gm, CHUNKS[0], here)
    up = Spread(wire, "up", 1, gu, CHUNKS[1], here)
    down = Spread(wire, "dn", 2, gd, CHUNKS[2], here)
    ag1 = Gather(wire, "tok", tokb, row)
    ag2 = [Gather(wire, ("aft", k), aftb.at[k], row) for k in (0, 1)]
    rs1, rs2 = (
        [Sum(wire, (name, k), row, *(ref.at[k] for ref in refs)) for k in (0, 1)]
        for name, refs in (
            ("rs1", (part1, pair1, stage1, mid1, end1)),
            ("rs2", (part2, pair2, stage2, mid2, end2)),
        )
    )

    barrier = pltpu.get_barrier_semaphore()
    peers = [
        mix.neighbour(0, 1),
        mix.neighbour(0, -1),
        mix.neighbour(1, 1),
        mix.neighbour(1, -1),
        row.dev(row.right),
        row.dev(row.left),
        row.partner,
    ]
    for peer in peers:
        pl.semaphore_signal(barrier, inc=1, device_id=peer, device_id_type=MESH)

    split = (2, 16)
    low, high = place(0), place(64)

    def ready(*which):
        for k in which:
            fetch[k].wait()

    def prepare():
        ready(0, 11, 12, 15)
        tokb[t] = tok[...].reshape(2, 128, 256)
        gu[z, y, :, :, 0:640] = ug[:, 0:640].reshape(*split, 640)
        gu[z, y, :, :, 640:1280] = uv[:, 0:640].reshape(*split, 640)
        tail = dot(ug[:, 640:704], low) + dot(uv[:, 640:704], high)
        gu[z, y, :, :, 1280:1408] = tail.astype(BF).reshape(*split, 128)
        gd[z, y, :, :, 0:640] = dn[:, 0:640].reshape(*split, 640)
        gd[z, y, :, :, 640:768] = dot(dn[:, 640:704], low).astype(BF).reshape(*split, 128)

    def start_norm():
        ready(*(k for k in range(16) if k not in FIRST))
        normed_into(nrm, (tokb,), gain1)

    ready(2, 3, 9)
    gm[z, y, :, :, 0:128] = wb[...].reshape(*split, 128)
    gm[z, y, :, :, 128:256] = wg[...].reshape(*split, 128)
    gm[z, y, :, :, 256:384] = wo[...].reshape(*split, 128)
    pl.semaphore_wait(barrier, len(peers))

    pos = lax.broadcasted_iota(jnp.int32, (SEQ, 128), 0)
    lane = lax.broadcasted_iota(jnp.int32, (SEQ, 128), 1)

    def project():
        w = gm[:, :, :, :, 0:256].reshape(2048, 256)
        pair[...] = dot(nrm[...], w).astype(BF)

    def recurrence():
        rmat = jnp.concatenate([dot(rmap[0], low), dot(rmap[1], high)], axis=0).astype(BF)
        imat = jnp.concatenate([dot(imap[0], low), dot(imap[1], high)], axis=0).astype(BF)
        for s in range(4):
            rows = slice(s * SEQ, (s + 1) * SEQ)
            cv = conv(f32(pair[rows, 0:128]), f32(taps1[...]), pos).astype(BF)
            recur = jax.nn.sigmoid(dot(cv, rmat))
            inner = jax.nn.sigmoid(dot(cv, imat))
            loga = -DECAY_RATE_GAIN * recur * rate[...].reshape(1, 128) + pld[rows, :]
            a = jnp.exp(loga)
            d = jnp.sqrt(jnp.tanh(-loga) * (1.0 + a * a)) * inner * f32(cv)
            k = 1
            while k < SEQ:
                d = d + a * shifted(d, k, pos)
                if 2 * k < SEQ:
                    a = a * shifted(a, k, pos, 1.0)
                k *= 2
            mixed[rows, :] = (d * jax.nn.gelu(f32(pair[rows, 128:256]))).astype(BF)

    def mixer_out(k):
        for j in range(N):
            w = gm[j, 4 * k : 4 * k + 4, :, :, 256:384].reshape(128, 128)
            part1[k, j % 2, j // 2] = dot_t(mixed[...], w).astype(BF)

    def residual(k):
        cols = pl.ds(k * 128, 128)
        for half in (0, 1):
            rows = pl.ds(half * 128, 128)
            aftb[k, t, half] = (f32(tok[rows, cols]) + rs1[k].total(half)).astype(BF)

    def expand(k):
        cols = pl.ds(k * 256, 256 if k < 5 else 128)
        w = gu[:, :, :, :, cols]
        gv[:, cols] = dot(nrm[...], w.reshape(2048, w.shape[-1])).astype(BF)

    def gated():
        tail_taps = dot(gtaps[:, 640:704], low) + dot(vtaps[:, 640:704], high)
        for s in range(4):
            rows = pl.ds(s * SEQ, SEQ)
            for k in range(5):
                cols = pl.ds(k * 128, 128)
                g = conv(f32(gv[rows, cols]), f32(gtaps[:, cols]), pos)
                v = conv(f32(gv[rows, pl.ds(640 + k * 128, 128)]), f32(vtaps[:, cols]), pos)
                hid[rows, cols] = (jax.nn.silu(g) * v).astype(BF)
            b = conv(f32(gv[rows, pl.ds(1280, 128)]), tail_taps, pos)
            h = jnp.where(lane < 64, jax.nn.silu(b) * pltpu.roll(b, 64, 1), 0.0)
            hid[rows, pl.ds(640, 128)] = h.astype(BF)

    def contract(late):
        for q in (N // 2,) if late else [q for q in range(N) if q != N // 2]:
            j = lax.rem(z + q, N)
            sums = dot_t(hid[...], gd[j].reshape(256, 768)).astype(BF)
            for k in (0, 1):
                part2[k, lax.rem(j, 2), j // 2] = sums[:, k * 128 : k * 128 + 128]

    def result(k):
        cols = pl.ds(k * 128, 128)
        for half in (0, 1):
            rows = pl.ds(half * 128, 128)
            final[k, rows, :] = (f32(aftb[k, t, half]) + rs2[k].total(half)).astype(BF)
        pltpu.make_async_copy(final.at[k], out.at[:, cols], in_sem.at[k]).start()

    spreads = {MIX: mix, UP: up, DN: down}
    steps = {
        (NORM1,): start_norm,
        (WIN,): project,
        (MIXER,): recurrence,
        (NORM2,): lambda: normed_into(nrm, (aftb.at[0], aftb.at[1]), gain2),
        (HID,): gated,
        (PART2, 0): lambda: contract(False),
        (PART2, 1): lambda: contract(True),
    }
    for k in range(6):
        steps[UPDOT, k] = functools.partial(expand, k)
    for k in (0, 1):
        steps[PART1, k] = functools.partial(mixer_out, k)
        steps[RS1, TOTAL, k] = functools.partial(residual, k)
        steps[RS2, TOTAL, k] = functools.partial(result, k)
    for name, k, gather in ((AG1, 0, ag1), (AG2, 0, ag2[0]), (AG2, 1, ag2[1])):
        steps[name, START, k] = gather.start
        steps[name, RELAY, k] = gather.relay
        steps[name, SHARE, k] = gather.share
        steps[name, SHAREFAR, k] = gather.share_far
        steps[name, DONE, k] = gather.done
    for name, parts in ((RS1, rs1), (RS2, rs2)):
        for k in (0, 1):
            steps[name, START, k] = parts[k].start
            steps[name, SPREAD, k] = parts[k].spread
            steps[name, REST, k] = parts[k].rest
            steps[name, RELAY, k] = parts[k].relay
    prepared = False
    for step in ORDER:
        if not prepared and step[0] != MIX:
            prepare()
            prepared = True
        if step[0] not in spreads:
            steps[step]()
            continue
        spread, what, rest = spreads[step[0]], step[1], step[2:]
        if what == S1:
            spread.pass1(1)
        elif what == F1:
            spread.forward1(*rest)
        elif what == S2:
            spread.pass2(*rest, 1)
        else:
            spread.forward2(*rest)
    for part in (mix, up, down, ag1, *ag2, *rs1, *rs2):
        part.finish()
    for k in (0, 1):
        cols = pl.ds(k * 128, 128)
        pltpu.make_async_copy(final.at[k], out.at[:, cols], in_sem.at[k]).wait()


def per_device(*args):
    (tok, gain1, wb, wg, taps1, rmap, imap, rate, pld, wo, gain2, ug, uv, gtaps, vtaps, dn) = args
    sums = [
        pltpu.VMEM((2, 2, X, 256, 128), BF),
        pltpu.VMEM((2, X, 256, 128), BF),
        pltpu.VMEM((2, 6, 128, 128), BF),
        pltpu.VMEM((2, 2, 128, 128), BF),
        pltpu.VMEM((2, 2, 2, 128, 128), BF),
    ]
    operands = (
        tok, gain1, wb, wg, taps1, rmap, imap, rate, pld, wo.T, gain2, ug, uv, gtaps, vtaps, dn.T
    )
    return pl.pallas_call(
        kernel,
        out_shape=jax.ShapeDtypeStruct((256, 256), BF),
        in_specs=[pl.BlockSpec(memory_space=pltpu.HBM)] * 16,
        out_specs=pl.BlockSpec(memory_space=pltpu.HBM),
        scratch_shapes=[
            *[pltpu.VMEM(a.shape, a.dtype) for a in operands],
            pltpu.SemaphoreType.DMA((16,)),
            pltpu.VMEM((N, N, 2, 16, 384), BF),
            pltpu.VMEM((N, N, 2, 16, 1408), BF),
            pltpu.VMEM((N, N, 2, 16, 768), BF),
            pltpu.VMEM((N, 2, 128, 256), BF),
            pltpu.VMEM((2, N, 2, 128, 128), BF),
            pltpu.VMEM((256, 2048), BF),
            pltpu.VMEM((256, 256), BF),
            pltpu.VMEM((256, 128), BF),
            pltpu.VMEM((256, 1408), BF),
            pltpu.VMEM((256, 768), BF),
            *sums,
            *sums,
            pltpu.VMEM((2, 256, 128), BF),
            pltpu.SemaphoreType.DMA((SENDS,)),
            pltpu.SemaphoreType.DMA((ARRIVALS,)),
        ],
        compiler_params=pltpu.CompilerParams(
            collective_id=0, has_side_effects=True, vmem_limit_bytes=67043328
        ),
        name="layer",
    )(*operands)


def solution(mesh):
    torus = Mesh(mesh.devices.reshape(N, N, mesh.shape["tp"]), ("fs_0", "fs_1", "tp"))
    return jax.shard_map(
        per_device,
        mesh=torus,
        in_specs=(
            P(FS, "tp"),
            P(),
            P(FS, "tp"),
            P(FS, "tp"),
            P(None, "tp"),
            P("tp", None, None),
            P("tp", None, None),
            P("tp"),
            P(FS, "tp"),
            P("tp", FS),
            P(),
            P(FS, "tp"),
            P(FS, "tp"),
            P(None, "tp"),
            P(None, "tp"),
            P("tp", FS),
        ),
        out_specs=P(FS, "tp"),
        check_vma=False,
    )
```

```python
import functools

import jax
import jax.numpy as jnp
from jax import lax
from jax.experimental import pallas as pl
from jax.experimental.pallas import tpu as pltpu
from jax.sharding import Mesh
from jax.sharding import PartitionSpec as P

SEQ = 64
FS = ("fs_0", "fs_1")
EPS = 1e-06
DECAY_RATE_GAIN = 8.0
BF = jnp.bfloat16
F32 = jnp.float32
MESH = pl.DeviceIdType.MESH
N = 8
X = 4
MIX, UP, DN, AG1, AG2, RS1, RS2 = range(7)
NORM1, WIN, MIXER, PART1, NORM2, UPDOT, HID, PART2 = range(7, 15)
S1, F1, S2, F2, START, RELAY, SHARE, SHAREFAR, DONE, SPREAD, REST, TOTAL = range(12)
SENDS = 14
ARRIVALS = 120
CHUNKS = (4, 8, 8)
ORDER = (
    (MIX, S1),
    (DN, S1),
    (UP, S1),
    (DN, S2, 0),
    (UP, S2, 0),
    (MIX, F1, 1),
    (MIX, S2, 0),
    (DN, F1, 1),
    (DN, S2, 1),
    (UP, F1, 1),
    (DN, F2, 0, 1),
    (AG1, START, 0),
    (UP, S2, 1),
    (MIX, F1, 2),
    (UP, S2, 7),
    (UP, F2, 0, 1),
    (MIX, F2, 0, 1),
    (UP, F1, 2),
    (MIX, F1, 3),
    (DN, F1, 2),
    (MIX, S2, 1),
    (AG1, RELAY, 0),
    (MIX, S2, 3),
    (UP, F2, 1, 1),
    (UP, S2, 2),
    (MIX, F2, 0, 2),
    (MIX, F1, 4),
    (MIX, S2, 2),
    (MIX, F2, 1, 1),
    (MIX, F2, 3, 1),
    (DN, F1, 3),
    (UP, F2, 7, 1),
    (DN, S2, 6),
    (UP, F1, 3),
    (MIX, F2, 2, 1),
    (AG1, SHARE, 0),
    (AG1, SHAREFAR, 0),
    (MIX, F2, 0, 3),
    (DN, F2, 1, 1),
    (MIX, F2, 1, 2),
    (MIX, F2, 3, 2),
    (UP, S2, 5),
    (DN, S2, 7),
    (UP, F1, 4),
    (MIX, F2, 2, 2),
    (UP, F2, 2, 1),
    (UP, S2, 3),
    (MIX, F2, 1, 3),
    (MIX, F2, 3, 3),
    (MIX, F2, 0, 4),
    (UP, S2, 4),
    (DN, F1, 4),
    (AG1, DONE, 0),
    (MIX, F2, 2, 3),
    (UP, S2, 6),
    (NORM1,),
    (DN, F2, 7, 1),
    (UP, F2, 5, 1),
    (UP, F2, 3, 1),
    (UP, F2, 7, 2),
    (DN, S2, 2),
    (MIX, F2, 1, 4),
    (DN, S2, 4),
    (UP, F2, 4, 1),
    (MIX, F2, 3, 4),
    (UP, F2, 1, 2),
    (MIX, F2, 2, 4),
    (WIN,),
    (MIXER,),
    (PART1, 1),
    (RS1, START, 1),
    (PART1, 0),
    (RS1, START, 0),
    (RS1, SPREAD, 1),
    (DN, S2, 5),
    (UP, F2, 6, 1),
    (RS1, SPREAD, 0),
    (UP, F2, 0, 2),
    (DN, S2, 3),
    (UP, F2, 3, 2),
    (RS1, REST, 0),
    (RS1, REST, 1),
    (UP, F2, 5, 2),
    (RS1, RELAY, 1),
    (UP, F2, 4, 2),
    (RS1, RELAY, 0),
    (UP, F2, 2, 2),
    (UP, F2, 6, 2),
    (RS1, TOTAL, 1),
    (AG2, START, 1),
    (DN, F2, 2, 1),
    (DN, F2, 6, 1),
    (UP, F2, 3, 3),
    (DN, F2, 3, 1),
    (UP, F2, 1, 3),
    (DN, F2, 5, 1),
    (RS1, TOTAL, 0),
    (AG2, START, 0),
    (UP, F2, 0, 3),
    (UP, F2, 2, 3),
    (AG2, RELAY, 1),
    (UP, F2, 6, 3),
    (UP, F2, 7, 3),
    (AG2, RELAY, 0),
    (UP, F2, 4, 3),
    (UP, F2, 5, 3),
    (DN, F2, 4, 1),
    (DN, F2, 1, 2),
    (AG2, SHARE, 0),
    (DN, F2, 6, 2),
    (DN, F2, 0, 2),
    (DN, F2, 7, 2),
    (AG2, SHARE, 1),
    (UP, F2, 3, 4),
    (DN, F2, 2, 2),
    (UP, F2, 1, 4),
    (DN, F2, 3, 2),
    (AG2, SHAREFAR, 1),
    (DN, F2, 5, 2),
    (AG2, SHAREFAR, 0),
    (AG2, DONE, 1),
    (UP, F2, 0, 4),
    (UP, F2, 2, 4),
    (UP, F2, 5, 4),
    (UP, F2, 6, 4),
    (UP, F2, 4, 4),
    (UP, F2, 7, 4),
    (DN, F2, 4, 2),
    (AG2, DONE, 0),
    (NORM2,),
    (UPDOT, 5),
    (DN, F2, 1, 3),
    (DN, F2, 6, 3),
    (UPDOT, 4),
    (DN, F2, 0, 3),
    (DN, F2, 7, 3),
    (DN, F2, 2, 3),
    (UPDOT, 0),
    (DN, F2, 3, 3),
    (DN, F2, 5, 3),
    (UPDOT, 1),
    (DN, F2, 4, 3),
    (UPDOT, 2),
    (UPDOT, 3),
    (HID,),
    (DN, F2, 6, 4),
    (DN, F2, 1, 4),
    (DN, F2, 0, 4),
    (DN, F2, 3, 4),
    (DN, F2, 2, 4),
    (DN, F2, 7, 4),
    (DN, F2, 5, 4),
    (PART2, 0),
    (DN, F2, 4, 4),
    (PART2, 1),
    (RS2, START, 0),
    (RS2, START, 1),
    (RS2, SPREAD, 0),
    (RS2, SPREAD, 1),
    (RS2, REST, 0),
    (RS2, REST, 1),
    (RS2, RELAY, 0),
    (RS2, RELAY, 1),
    (RS2, TOTAL, 0),
    (RS2, TOTAL, 1),
)
FIRST = (2, 3, 9, 0, 11, 12, 15)


def f32(v):
    return v.astype(F32)


def dot(a, b):
    return jnp.dot(a, b, preferred_element_type=F32)


def dot_t(a, b):
    return lax.dot_general(a, b, (((1,), (1,)), ((), ())), preferred_element_type=F32)


def place(offset):
    r = lax.broadcasted_iota(jnp.int32, (64, 128), 0)
    c = lax.broadcasted_iota(jnp.int32, (64, 128), 1)
    return jnp.where(c == r + offset, 1.0, 0.0).astype(BF)


def shifted(v, k, row, fill=0.0):
    return jnp.where(row >= k, pltpu.roll(v, k, 0), fill)


def conv(v, taps, row):
    width = taps.shape[0]
    total = v * taps[width - 1 : width]
    for k in range(1, width):
        total = total + shifted(v, k, row) * taps[width - 1 - k : width - k]
    return total


class Wire:
    def __init__(self, send, recv):
        self.send, self.recv, self.sent, self.due = send, recv, {}, {}

    def go(self, group, key, src, dst, dev):
        out = self.sent.setdefault(group, len(self.sent))
        into = self.due.setdefault(key, len(self.due))
        pltpu.make_async_remote_copy(
            src_ref=src,
            dst_ref=dst,
            send_sem=self.send.at[out],
            recv_sem=self.recv.at[into],
            device_id=dev,
            device_id_type=MESH,
        ).start()

    def got(self, key, ref):
        pltpu.make_async_copy(ref, ref, self.recv.at[self.due[key]]).wait()

    def gone(self, group, ref):
        pltpu.make_async_copy(ref, ref, self.send.at[self.sent[group]]).wait()


class Spread:
    def __init__(self, wire, name, index, buf, chunks, here):
        self.wire, self.name, self.index, self.buf, self.chunks = wire, name, index, buf, chunks
        self.z, self.y, self.t = here

    def neighbour(self, axis, way):
        if axis == 0:
            return (lax.rem(self.z + N + way, N), self.y, self.t)
        return (self.z, lax.rem(self.y + N + way, N), self.t)

    def first(self, half, way, step):
        axis = 1 - half
        pos = lax.rem((self.y if axis else self.z) + N - way * (step - 1), N)
        return self.buf.at[self.z, pos, 0] if half == 0 else self.buf.at[pos, self.y, 1]

    def pass1(self, step):
        for half in (0, 1):
            for way in (1, -1):
                far = 1 if (self.index + half) % 2 == 0 else -1
                if step < N // 2 or (step == N // 2 and way == far):
                    ref = self.first(half, way, step)
                    dev = self.neighbour(1 - half, way)
                    self.wire.go(self.name, (self.name, step), ref, ref, dev)

    def forward1(self, step):
        self.wire.got((self.name, step), self.buf.at[0, pl.ds(0, 2 if step < N // 2 else 1)])
        self.pass1(step + 1)

    def second(self, half, way, step, q):
        size = N // self.chunks
        own = (self.z if half else self.y) // size
        part = pl.ds(lax.rem(own + q, self.chunks) * size, size)
        pos = lax.rem((self.y if half else self.z) + N - way * (step - 1), N)
        return self.buf.at[pos, part, 0] if half == 0 else self.buf.at[part, pos, 1]

    def pass2(self, q, step):
        far = 1 if q < self.chunks // 2 else -1
        for half in (0, 1):
            for way in (1, -1):
                if step < N // 2 or (step == N // 2 and way == far):
                    ref = self.second(half, way, step, q)
                    dev = self.neighbour(half, way)
                    self.wire.go(self.name, (self.name, step, q), ref, ref, dev)

    def forward2(self, q, step):
        size = N // self.chunks
        self.wire.got(
            (self.name, step, q), self.buf.at[0, pl.ds(0, 2 * size if step < N // 2 else size)]
        )
        self.pass2(q, step + 1)

    def finish(self):
        self.wire.gone(self.name, self.buf.reshape(N * N, *self.buf.shape[2:]).at[pl.ds(0, N * N - 1)])


class Row:
    def __init__(self, z, y, t):
        self.z, self.y, self.t = z, y, t
        self.x, self.c = t // 2, lax.rem(t, 2)
        self.right = lax.rem(self.x + 1, X)
        self.left = lax.rem(self.x + X - 1, X)
        self.across = lax.rem(self.x + 2, X)

    def dev(self, x):
        return (self.z, self.y, 2 * x + self.c)

    def same(self, x):
        return 2 * x + self.c

    @property
    def partner(self):
        return (self.z, self.y, 2 * self.x + 1 - self.c)


class Gather:
    def __init__(self, wire, name, buf, row):
        self.wire, self.name, self.buf, self.row = wire, name, buf, row

    def go(self, key, ref, dev):
        self.wire.go(self.name, (self.name, key), ref, ref, dev)

    def got(self, key, count):
        self.wire.got((self.name, key), self.buf.at[pl.ds(0, count)])

    def start(self):
        r, b = self.row, self.buf
        for k in (0, 1):
            self.go(k, b.at[r.t, k], r.dev(r.right))
            self.go(k, b.at[r.t, 1 - k], r.dev(r.left))
        self.go("pair", b.at[r.t], r.partner)

    def relay(self):
        r, b = self.row, self.buf
        self.got(0, 1)
        self.go("far", b.at[r.same(r.left), 0], r.dev(r.right))
        self.go("far", b.at[r.same(r.right), 1], r.dev(r.left))

    def share(self):
        r, b = self.row, self.buf
        self.got(1, 1)
        self.go("pair", b.at[r.same(r.left)], r.partner)
        self.go("pair", b.at[r.same(r.right)], r.partner)

    def share_far(self):
        r, b = self.row, self.buf
        self.got("far", 1)
        self.go("pair", b.at[r.same(r.across)], r.partner)

    def done(self):
        self.got("pair", 4)

    def finish(self):
        self.wire.gone(self.name, self.buf.at[pl.ds(0, 7)])


class Sum:
    def __init__(self, wire, name, row, part, pair, stage, mid, end):
        self.wire, self.name, self.row = wire, name, row
        self.part, self.pair, self.stage, self.mid, self.end = part, pair, stage, mid, end

    def key(self, k):
        return (self.name, k)

    def start(self):
        r = self.row
        for x, key in ((r.across, 0), (r.right, 3), (r.left, 3), (r.x, 3)):
            src, dst = self.part.at[1 - r.c, x], self.pair.at[x]
            self.wire.go(self.key(0), self.key(key), src, dst, r.partner)

    def both(self, x, half):
        rows = pl.ds(half * 128, 128)
        return f32(self.part[self.row.c, x, rows, :]) + f32(self.pair[x, rows, :])

    def out(self, k, value, dst, way):
        r = self.row
        self.stage[k] = value.astype(BF)
        dev = r.dev(r.right if way == 1 else r.left)
        self.wire.go(self.key(1), self.key(1 if k < 2 else 2), self.stage.at[k], dst, dev)

    def spread(self):
        r = self.row
        self.wire.got(self.key(0), self.pair.at[0])
        self.out(0, self.both(r.across, 0), self.mid.at[0], 1)
        self.out(1, self.both(r.across, 1), self.mid.at[1], -1)

    def rest(self):
        r = self.row
        self.wire.got(self.key(3), self.pair.at[pl.ds(0, 3)])
        self.out(2, self.both(r.right, 1), self.end.at[0, 1], 1)
        self.out(3, self.both(r.left, 0), self.end.at[1, 0], -1)

    def relay(self):
        r = self.row
        self.wire.got(self.key(1), self.mid)
        self.out(4, self.both(r.right, 0) + f32(self.mid[0]), self.end.at[0, 0], 1)
        self.out(5, self.both(r.left, 1) + f32(self.mid[1]), self.end.at[1, 1], -1)

    def total(self, half):
        r = self.row
        if half == 0:
            self.wire.got(self.key(2), self.end)
        return self.both(r.x, half) + f32(self.end[0, half]) + f32(self.end[1, half])

    def finish(self):
        self.wire.gone(self.key(0), self.pair)
        self.wire.gone(self.key(1), self.stage)


def normed_into(out, bufs, gain):
    width = 256 // len(bufs)
    for half in (0, 1):
        for part in (0, 1):
            rows = pl.ds(part * 64, 64)
            sums = jnp.zeros((64, width), F32)
            for j in range(N):
                for buf in bufs:
                    v = f32(buf[j, half, rows, :])
                    sums = sums + v * v
            mean = jnp.sum(sums, axis=1, keepdims=True) * (1.0 / (N * 256))
            factor = lax.rsqrt(mean + EPS)
            for j in range(N):
                for k, buf in enumerate(bufs):
                    v = f32(buf[j, half, rows, :])
                    cols = pl.ds(j * 256 + k * width, width)
                    scale = f32(gain[cols].reshape(1, width))
                    out[pl.ds(half * 128 + part * 64, 64), cols] = (v * factor * scale).astype(BF)


def kernel(*refs):
    sources, refs = refs[:16], refs[16:]
    out, staged, in_sem, refs = refs[0], refs[1:17], refs[17], refs[18:]
    fetch = [
        pltpu.make_async_copy(source, target, in_sem.at[k])
        for k, (source, target) in enumerate(zip(sources, staged))
    ]
    for k in FIRST:
        fetch[k].start()
    for k in range(16):
        if k not in FIRST:
            fetch[k].start()
    body(fetch, in_sem, out, *staged, *refs)


def body(
    fetch,
    in_sem,
    out,
    tok,
    gain1,
    wb,
    wg,
    taps1,
    rmap,
    imap,
    rate,
    pld,
    wo,
    gain2,
    ug,
    uv,
    gtaps,
    vtaps,
    dn,
    gm,
    gu,
    gd,
    tokb,
    aftb,
    nrm,
    pair,
    mixed,
    gv,
    hid,
    part1,
    pair1,
    stage1,
    mid1,
    end1,
    part2,
    pair2,
    stage2,
    mid2,
    end2,
    final,
    ssem,
    rsem,
):
    z, y, t = lax.axis_index("fs_0"), lax.axis_index("fs_1"), lax.axis_index("tp")
    here = (z, y, t)
    wire = Wire(ssem, rsem)
    row = Row(z, y, t)
    mix = Spread(wire, "mix", 0, gm, CHUNKS[0], here)
    up = Spread(wire, "up", 1, gu, CHUNKS[1], here)
    down = Spread(wire, "dn", 2, gd, CHUNKS[2], here)
    ag1 = Gather(wire, "tok", tokb, row)
    ag2 = [Gather(wire, ("aft", k), aftb.at[k], row) for k in (0, 1)]
    rs1, rs2 = (
        [Sum(wire, (name, k), row, *(ref.at[k] for ref in refs)) for k in (0, 1)]
        for name, refs in (
            ("rs1", (part1, pair1, stage1, mid1, end1)),
            ("rs2", (part2, pair2, stage2, mid2, end2)),
        )
    )

    barrier = pltpu.get_barrier_semaphore()
    peers = [
        mix.neighbour(0, 1),
        mix.neighbour(0, -1),
        mix.neighbour(1, 1),
        mix.neighbour(1, -1),
        row.dev(row.right),
        row.dev(row.left),
        row.partner,
    ]
    for peer in peers:
        pl.semaphore_signal(barrier, inc=1, device_id=peer, device_id_type=MESH)

    split = (2, 16)
    low, high = place(0), place(64)

    def ready(*which):
        for k in which:
            fetch[k].wait()

    def prepare():
        ready(0, 11, 12, 15)
        tokb[t] = tok[...].reshape(2, 128, 256)
        gu[z, y, :, :, 0:640] = ug[:, 0:640].reshape(*split, 640)
        gu[z, y, :, :, 640:1280] = uv[:, 0:640].reshape(*split, 640)
        tail = dot(ug[:, 640:704], low) + dot(uv[:, 640:704], high)
        gu[z, y, :, :, 1280:1408] = tail.astype(BF).reshape(*split, 128)
        gd[z, y, :, :, 0:640] = dn[:, 0:640].reshape(*split, 640)
        gd[z, y, :, :, 640:768] = dot(dn[:, 640:704], low).astype(BF).reshape(*split, 128)

    def start_norm():
        ready(*(k for k in range(16) if k not in FIRST))
        normed_into(nrm, (tokb,), gain1)

    ready(2, 3, 9)
    gm[z, y, :, :, 0:128] = wb[...].reshape(*split, 128)
    gm[z, y, :, :, 128:256] = wg[...].reshape(*split, 128)
    gm[z, y, :, :, 256:384] = wo[...].reshape(*split, 128)
    pl.semaphore_wait(barrier, len(peers))

    pos = lax.broadcasted_iota(jnp.int32, (SEQ, 128), 0)
    lane = lax.broadcasted_iota(jnp.int32, (SEQ, 128), 1)

    def project():
        w = gm[:, :, :, :, 0:256].reshape(2048, 256)
        pair[...] = dot(nrm[...], w).astype(BF)

    def recurrence():
        rmat = jnp.concatenate([dot(rmap[0], low), dot(rmap[1], high)], axis=0).astype(BF)
        imat = jnp.concatenate([dot(imap[0], low), dot(imap[1], high)], axis=0).astype(BF)
        for s in range(4):
            rows = slice(s * SEQ, (s + 1) * SEQ)
            cv = conv(f32(pair[rows, 0:128]), f32(taps1[...]), pos).astype(BF)
            recur = jax.nn.sigmoid(dot(cv, rmat))
            inner = jax.nn.sigmoid(dot(cv, imat))
            loga = -DECAY_RATE_GAIN * recur * rate[...].reshape(1, 128) + pld[rows, :]
            a = jnp.exp(loga)
            d = jnp.sqrt(jnp.tanh(-loga) * (1.0 + a * a)) * inner * f32(cv)
            k = 1
            while k < SEQ:
                d = d + a * shifted(d, k, pos)
                if 2 * k < SEQ:
                    a = a * shifted(a, k, pos, 1.0)
                k *= 2
            mixed[rows, :] = (d * jax.nn.gelu(f32(pair[rows, 128:256]))).astype(BF)

    def mixer_out(k):
        for j in range(N):
            w = gm[j, 4 * k : 4 * k + 4, :, :, 256:384].reshape(128, 128)
            part1[k, j % 2, j // 2] = dot_t(mixed[...], w).astype(BF)

    def residual(k):
        cols = pl.ds(k * 128, 128)
        for half in (0, 1):
            rows = pl.ds(half * 128, 128)
            aftb[k, t, half] = (f32(tok[rows, cols]) + rs1[k].total(half)).astype(BF)

    def expand(k):
        cols = pl.ds(k * 256, 256 if k < 5 else 128)
        w = gu[:, :, :, :, cols]
        gv[:, cols] = dot(nrm[...], w.reshape(2048, w.shape[-1])).astype(BF)

    def gated():
        tail_taps = dot(gtaps[:, 640:704], low) + dot(vtaps[:, 640:704], high)
        for s in range(4):
            rows = pl.ds(s * SEQ, SEQ)
            for k in range(5):
                cols = pl.ds(k * 128, 128)
                g = conv(f32(gv[rows, cols]), f32(gtaps[:, cols]), pos)
                v = conv(f32(gv[rows, pl.ds(640 + k * 128, 128)]), f32(vtaps[:, cols]), pos)
                hid[rows, cols] = (jax.nn.silu(g) * v).astype(BF)
            b = conv(f32(gv[rows, pl.ds(1280, 128)]), tail_taps, pos)
            h = jnp.where(lane < 64, jax.nn.silu(b) * pltpu.roll(b, 64, 1), 0.0)
            hid[rows, pl.ds(640, 128)] = h.astype(BF)

    def contract(late):
        for q in (N // 2,) if late else [q for q in range(N) if q != N // 2]:
            j = lax.rem(z + q, N)
            sums = dot_t(hid[...], gd[j].reshape(256, 768)).astype(BF)
            for k in (0, 1):
                part2[k, lax.rem(j, 2), j // 2] = sums[:, k * 128 : k * 128 + 128]

    def result(k):
        cols = pl.ds(k * 128, 128)
        for half in (0, 1):
            rows = pl.ds(half * 128, 128)
            final[k, rows, :] = (f32(aftb[k, t, half]) + rs2[k].total(half)).astype(BF)
        pltpu.make_async_copy(final.at[k], out.at[:, cols], in_sem.at[k]).start()

    spreads = {MIX: mix, UP: up, DN: down}
    steps = {
        (NORM1,): start_norm,
        (WIN,): project,
        (MIXER,): recurrence,
        (NORM2,): lambda: normed_into(nrm, (aftb.at[0], aftb.at[1]), gain2),
        (HID,): gated,
        (PART2, 0): lambda: contract(False),
        (PART2, 1): lambda: contract(True),
    }
    for k in range(6):
        steps[UPDOT, k] = functools.partial(expand, k)
    for k in (0, 1):
        steps[PART1, k] = functools.partial(mixer_out, k)
        steps[RS1, TOTAL, k] = functools.partial(residual, k)
        steps[RS2, TOTAL, k] = functools.partial(result, k)
    for name, k, gather in ((AG1, 0, ag1), (AG2, 0, ag2[0]), (AG2, 1, ag2[1])):
        steps[name, START, k] = gather.start
        steps[name, RELAY, k] = gather.relay
        steps[name, SHARE, k] = gather.share
        steps[name, SHAREFAR, k] = gather.share_far
        steps[name, DONE, k] = gather.done
    for name, parts in ((RS1, rs1), (RS2, rs2)):
        for k in (0, 1):
            steps[name, START, k] = parts[k].start
            steps[name, SPREAD, k] = parts[k].spread
            steps[name, REST, k] = parts[k].rest
            steps[name, RELAY, k] = parts[k].relay
    prepared = False
    for step in ORDER:
        if not prepared and step[0] != MIX:
            prepare()
            prepared = True
        if step[0] not in spreads:
            steps[step]()
            continue
        spread, what, rest = spreads[step[0]], step[1], step[2:]
        if what == S1:
            spread.pass1(1)
        elif what == F1:
            spread.forward1(*rest)
        elif what == S2:
            spread.pass2(*rest, 1)
        else:
            spread.forward2(*rest)
    for part in (mix, up, down, ag1, *ag2, *rs1, *rs2):
        part.finish()
    for k in (0, 1):
        cols = pl.ds(k * 128, 128)
        pltpu.make_async_copy(final.at[k], out.at[:, cols], in_sem.at[k]).wait()


def per_device(*args):
    (tok, gain1, wb, wg, taps1, rmap, imap, rate, pld, wo, gain2, ug, uv, gtaps, vtaps, dn) = args
    sums = [
        pltpu.VMEM((2, 2, X, 256, 128), BF),
        pltpu.VMEM((2, X, 256, 128), BF),
        pltpu.VMEM((2, 6, 128, 128), BF),
        pltpu.VMEM((2, 2, 128, 128), BF),
        pltpu.VMEM((2, 2, 2, 128, 128), BF),
    ]
    operands = (
        tok, gain1, wb, wg, taps1, rmap, imap, rate, pld, wo.T, gain2, ug, uv, gtaps, vtaps, dn.T
    )
    return pl.pallas_call(
        kernel,
        out_shape=jax.ShapeDtypeStruct((256, 256), BF),
        in_specs=[pl.BlockSpec(memory_space=pltpu.HBM)] * 16,
        out_specs=pl.BlockSpec(memory_space=pltpu.HBM),
        scratch_shapes=[
            *[pltpu.VMEM(a.shape, a.dtype) for a in operands],
            pltpu.SemaphoreType.DMA((16,)),
            pltpu.VMEM((N, N, 2, 16, 384), BF),
            pltpu.VMEM((N, N, 2, 16, 1408), BF),
            pltpu.VMEM((N, N, 2, 16, 768), BF),
            pltpu.VMEM((N, 2, 128, 256), BF),
            pltpu.VMEM((2, N, 2, 128, 128), BF),
            pltpu.VMEM((256, 2048), BF),
            pltpu.VMEM((256, 256), BF),
            pltpu.VMEM((256, 128), BF),
            pltpu.VMEM((256, 1408), BF),
            pltpu.VMEM((256, 768), BF),
            *sums,
            *sums,
            pltpu.VMEM((2, 256, 128), BF),
            pltpu.SemaphoreType.DMA((SENDS,)),
            pltpu.SemaphoreType.DMA((ARRIVALS,)),
        ],
        compiler_params=pltpu.CompilerParams(
            collective_id=0, has_side_effects=True, vmem_limit_bytes=67043328
        ),
        name="layer",
    )(*operands)


def solution(mesh):
    torus = Mesh(mesh.devices.reshape(N, N, mesh.shape["tp"]), ("fs_0", "fs_1", "tp"))
    return jax.shard_map(
        per_device,
        mesh=torus,
        in_specs=(
            P(FS, "tp"),
            P(),
            P(FS, "tp"),
            P(FS, "tp"),
            P(None, "tp"),
            P("tp", None, None),
            P("tp", None, None),
            P("tp"),
            P(FS, "tp"),
            P("tp", FS),
            P(),
            P(FS, "tp"),
            P(FS, "tp"),
            P(None, "tp"),
            P(None, "tp"),
            P("tp", FS),
        ),
        out_specs=P(FS, "tp"),
        check_vma=False,
    )
```
